32 devices in a mesh: sp: 8 (over z, x), dp: 4 (over y, core).
Axes of the slice: x: 2, y: 2, z: 4, core: 2. Of those that a mesh axis runs over, the one named last changes fastest.
Arguments:
- queries: bfloat16 [4, 1024, 2048], P('dp', 'sp'), may hold values from -6 to 6
- keys: bfloat16 [4, 1024, 2048], P('dp', 'sp'), may hold values from -6 to 6
- values: bfloat16 [4, 1024, 2048], P('dp', 'sp'), may hold values from -6 to 6
- gate_totals: float32 [4, 1024, 32], P('dp', 'sp'), may hold values from -1024 to 0, as said below
- w_out: bfloat16 [2048, 2048], P(None, 'dp'), may hold values from -1 to 1
Outputs:
- mixed: bfloat16 [4, 1024, 2048], P('dp', 'sp')
The draws below stay inside these ranges and needn't reach their ends.
Inputs may be any that keep to these rules, and one draw needn't show every extreme that they name: `gate_totals`: never rising along a sequence.
All inputs are finite; a program needn't handle non-finite values.
Results may differ from the reference program's by a relative error of at most 0.0053.
Values may be sent and summed in bfloat16 or wider, within the bound.
A program may use at most 64 MiB of HBM per device.

```python
import math
import jax
import jax.numpy as jnp
from jax import lax

D = 2048
HEADS = 32
HEAD_DIM = 64
ATTN = 2048
LENGTH = 1024
BATCH = 4


def paired_draw(key):
    base = jax.random.fold_in(key, 11)
    first, second = jax.random.split(base, 2)
    shape = (BATCH, LENGTH, ATTN)
    query_draw = jnp.clip(jax.random.normal(first, shape, jnp.float32), -6.0, 6.0)
    key_draw = jnp.clip(jax.random.normal(second, shape, jnp.float32), -6.0, 6.0)
    return (query_draw, key_draw)


def draw_queries(key, part):
    return paired_draw(key)[0].astype(jnp.bfloat16)


def draw_keys(key, part):
    return paired_draw(key)[1].astype(jnp.bfloat16)


def draw_gate_totals(key, part):
    base = jax.random.fold_in(key, 23)
    first, second, third = jax.random.split(base, 3)
    fast_share = 0.5
    fast_heads = jax.random.bernoulli(first, fast_share, (BATCH, 1, HEADS))
    rates = jnp.where(fast_heads, 0.075, 1.2 / LENGTH).astype(jnp.float32)
    rough = jax.random.uniform(second, (BATCH, LENGTH, HEADS), jnp.float32, 0.3, 1.7)
    blocks = (LENGTH + 63) // 64
    block_scale = jnp.exp(jax.random.uniform(third, (BATCH, blocks, 1), jnp.float32, math.log(0.4), math.log(2.5)))
    block_scale = jnp.repeat(block_scale, 64, axis=1)[:, :LENGTH]
    log_gates = -rates * rough * block_scale
    return jnp.cumsum(log_gates, axis=1)


def level_of(stream_key, shape, cuts, least, top_value):
    level = 1.0
    for axis_at, parts in cuts:
        heights = jax.random.uniform(jax.random.fold_in(jax.random.fold_in(stream_key, 6), axis_at), (parts,), jnp.float32, least / len(cuts), top_value / len(cuts))
        level = level * jnp.repeat(jnp.exp(heights), shape[axis_at] // parts).reshape((-1,) + (1,) * (len(shape) - 1 - axis_at))
    return level


def bell_draw(stream_key, extent, width, bound, cuts=(), dtype=jnp.bfloat16):
    gain = level_of(stream_key, extent, cuts, -0.22, 0.18) if cuts else 1.0
    drawn = jax.random.normal(stream_key, extent, jnp.float32) * width * gain
    return jnp.minimum(jnp.maximum(drawn, -bound), bound).astype(dtype)


def setup_inputs(seed: int = 0) -> dict:
    splits = jax.random.split(jax.random.key(seed), 6)
    return {
        "queries": draw_queries(jax.random.fold_in(splits[5], 71), 0),
        "keys": draw_keys(jax.random.fold_in(splits[5], 71), 0),
        "values": bell_draw(splits[2], (BATCH, LENGTH, ATTN), 1.0, 6.0, ((0, 4), (1, 8))),
        "gate_totals": draw_gate_totals(jax.random.fold_in(splits[5], 71), 0),
        "w_out": bell_draw(splits[4], (ATTN, D), HEADS ** -0.5, 1.0, ((1, 4),)),
    }


def attend(queries, key_rows, value_rows, totals):
    length = queries.shape[0]
    block_rows = min(length, 512)
    pieces = []
    for begin_row in range(0, length, block_rows):
        end_row = begin_row + block_rows
        scores = jnp.einsum('qhd,khd->hqk', queries[begin_row:end_row].astype(jnp.float32), key_rows[:end_row].astype(jnp.float32)) * HEAD_DIM ** -0.5
        scores = scores + jnp.transpose(totals[begin_row:end_row])[:, :, None] - jnp.transpose(totals[:end_row])[:, None, :]
        causal = jnp.arange(end_row)[None, :] <= (begin_row + jnp.arange(block_rows))[:, None]
        scores = jnp.where(causal[None], scores, -jnp.inf)
        biggest = jnp.max(scores, axis=-1, keepdims=True)
        expo = jnp.exp(scores - biggest)
        summed = jnp.sum(expo, axis=-1)
        weights = expo.astype(jnp.bfloat16).astype(jnp.float32)
        output = jnp.einsum('hqk,khd->qhd', weights, value_rows[:end_row].astype(jnp.float32))
        output = output / jnp.transpose(summed)[:, :, None]
        pieces.append(output.astype(jnp.bfloat16))
    return jnp.concatenate(pieces, axis=0).reshape(length, -1)


def reference(queries, keys, values, gate_totals, w_out):
    shape4 = (BATCH, LENGTH, HEADS, HEAD_DIM)

    def one_sequence(items):
        return attend(items[0], items[1], items[2], items[3])

    attended = lax.map(one_sequence, (queries.reshape(shape4), keys.reshape(shape4), values.reshape(shape4), gate_totals))
    mixed = jnp.dot(attended.reshape(BATCH * LENGTH, ATTN), w_out, preferred_element_type=jnp.float32)
    return mixed.astype(jnp.bfloat16).reshape(BATCH, LENGTH, D)
```

```python
import functools

import jax
import jax.numpy as jnp
from jax import lax
from jax.experimental import pallas as pl
from jax.experimental.pallas import tpu as pltpu
from jax.sharding import PartitionSpec as P

HEAD_DIM = 64
LANES = 128
W_CHUNKS = 16
MESH = pl.DeviceIdType.MESH


def attend(queries, key_rows, value_rows, totals):
    length = queries.shape[0]
    block_rows = min(length, 512)
    pieces = []
    for begin_row in range(0, length, block_rows):
        end_row = begin_row + block_rows
        scaled = queries[begin_row:end_row] * jnp.bfloat16(HEAD_DIM ** (-0.5))
        scores = jnp.einsum(
            "qhd,khd->hqk", scaled, key_rows[:end_row], preferred_element_type=jnp.float32
        )
        causal = jnp.arange(end_row)[None, :] <= (begin_row + jnp.arange(block_rows))[:, None]
        scores = jnp.where(
            causal[None],
            scores
            + jnp.transpose(totals[begin_row:end_row])[:, :, None]
            - jnp.transpose(totals[:end_row])[:, None, :],
            -jnp.inf,
        )
        biggest = jnp.max(scores, axis=-1, keepdims=True)
        expo = jnp.exp(scores - biggest)
        summed = jnp.sum(expo, axis=-1)
        weights = expo.astype(jnp.bfloat16)
        output = jnp.einsum(
            "hqk,khd->qhd", weights, value_rows[:end_row], preferred_element_type=jnp.float32
        )
        output = output / jnp.transpose(summed)[:, :, None]
        pieces.append(output.astype(jnp.bfloat16))
    return jnp.concatenate(pieces, axis=0).reshape(length, -1)


def general(queries, keys, values, gate_totals, w_out):
    moved = [
        lax.all_to_all(x, "sp", split_axis=2, concat_axis=1, tiled=True)
        for x in (queries, keys, values, gate_totals)
    ]
    length = moved[0].shape[1]
    heads = [x[0].reshape(length, -1, HEAD_DIM) for x in moved[:3]]
    attended = attend(heads[0], heads[1], heads[2], moved[3][0])[None]
    rows = lax.all_to_all(attended, "sp", split_axis=1, concat_axis=2, tiled=True)
    mixed = jnp.dot(
        rows[0],
        lax.all_gather(w_out, "dp", axis=1, tiled=True),
        preferred_element_type=jnp.float32,
    )
    return mixed.astype(jnp.bfloat16)[None]


def attend_rows(queries, parts, diagonal):
    rows = queries.shape[0]
    scaled = queries * jnp.bfloat16(HEAD_DIM ** -0.5)
    lane = lax.broadcasted_iota(jnp.int32, (rows, LANES), 1)
    outs, sums = [], []
    for h in range(2):
        mine = (lane < HEAD_DIM) if h == 0 else (lane >= HEAD_DIM)
        scores = []
        for at, (keys, _, gates) in enumerate(parts):
            head_keys = jnp.where(mine, keys, jnp.zeros_like(keys))
            score = lax.dot_general(
                scaled, head_keys, (((1,), (1,)), ((), ())), preferred_element_type=jnp.float32)
            score = score - gates[h:h + 1, :]
            if diagonal and at == len(parts) - 1:
                causal = lax.broadcasted_iota(jnp.int32, score.shape, 1) <= lax.broadcasted_iota(
                    jnp.int32, score.shape, 0)
                score = jnp.where(causal, score, -jnp.inf)
            scores.append(score)
        peak = functools.reduce(jnp.maximum, [jnp.max(x, axis=1, keepdims=True) for x in scores])
        expo = [jnp.exp(x - peak) for x in scores]
        total = sum(jnp.sum(x, axis=1, keepdims=True) for x in expo)
        out = sum(
            jnp.dot(x.astype(jnp.bfloat16), part[1], preferred_element_type=jnp.float32)
            for x, part in zip(expo, parts))
        outs.append(out / total)
        sums.append(peak + jnp.log(total))
    first = lane < HEAD_DIM
    return jnp.where(first, outs[0], outs[1]), jnp.where(first, sums[0], sums[1])


def kernel(n, ndp, q_ref, k_ref, v_ref, g_ref, w_ref, o_ref,
           qx, kx, vx, kz, vz, qz, gb, ob, held_o, held_l, part_o, part_l, got_o, got_l, att, wall, acc,
           x_send, x_recv, g_send, g_recv, own_sem, w_sem, z_send, z_recv, po_send, po_recv, pl_send, pl_recv,
           o_send, o_recv, y_send, y_recv, wx_send, wx_recv, p_send, p_recv, f_send, f_recv):
    me = lax.axis_index("sp")
    x = lax.rem(me, 2)
    z = lax.div(me, 2)
    side = me + 1 - 2 * x
    me_dp = lax.axis_index("dp")
    core = lax.rem(me_dp, 2)
    row_y = lax.div(me_dp, 2)
    across = (1 - row_y) * 2 + core
    partner = row_y * 2 + 1 - core
    L = q_ref.shape[0]
    pairs = qx.shape[0]
    W = pairs * LANES
    w_cols = w_ref.shape[3]
    units = 3 * pairs // 4
    quarter = pairs // 4

    barrier = pltpu.get_barrier_semaphore()
    meets = {0: (1,), 1: (0, 2, 3), 2: (1, 3), 3: (1, 2)}
    for here, others in meets.items():
        @pl.when(z == here)
        def _(others=others):
            for other in others:
                pl.semaphore_signal(barrier, inc=1, device_id={"sp": other * 2 + x}, device_id_type=MESH)
    pl.semaphore_signal(barrier, inc=1, device_id={"sp": side}, device_id_type=MESH)
    for other in (partner, across):
        pl.semaphore_signal(barrier, inc=1, device_id={"dp": other}, device_id_type=MESH)
    for here, others in meets.items():
        @pl.when(z == here)
        def _(others=others):
            pl.semaphore_wait(barrier, len(others) + 3)

    def remote(src, dst, send, recv, **device):
        return pltpu.make_async_remote_copy(
            src_ref=src, dst_ref=dst, send_sem=send, recv_sem=recv, device_id=device, device_id_type=MESH)

    def rows_of(which):
        return pl.ds(pl.multiple_of(which * L, L), L)

    def lanes_of(which, p):
        return pl.ds(pl.multiple_of(which * W + p * LANES, LANES), LANES)

    def half_of(which):
        return pl.ds(pl.multiple_of(which * LANES, LANES), LANES)

    bufs = ((q_ref, qx), (k_ref, kx), (v_ref, vx))

    def x_copy(a, p):
        src, dst = bufs[a]
        return remote(src.at[:, lanes_of(1 - x, p)], dst.at[p, rows_of(x), :],
                      x_send.at[a, p], x_recv.at[a, p], sp=side)

    def x_own(a, p):
        src, dst = bufs[a]
        return pltpu.make_async_copy(src.at[:, lanes_of(x, p)], dst.at[p, rows_of(x), :], own_sem.at[a, p])

    g_copy = remote(g_ref.at[1 - x], gb.at[me], g_send.at[0], g_recv.at[0], sp=side)
    g_own = pltpu.make_async_copy(g_ref.at[x], gb.at[me], g_recv.at[1])

    def z_own(a, dst, k, slot, p, target):
        src = bufs[a][0]
        return remote(src.at[:, lanes_of(x, p)], dst.at[rows_of(x), :],
                      z_send.at[k, x, p], z_recv.at[slot, x, p], sp=target * 2 + x)

    def z_side(a, dst, k, slot, p, target):
        src = bufs[a][1]
        return remote(src.at[p, rows_of(1 - x), :], dst.at[rows_of(1 - x), :],
                      z_send.at[k, 1 - x, p], z_recv.at[slot, 1 - x, p], sp=target * 2 + x)

    def z_arrived(a, dst, slot, p):
        z_own(a, dst, 0, slot, p, 0).wait_recv()
        z_side(a, dst, 0, slot, p, 0).wait_recv()

    def z_sent(a, dst, k, slot, p, target):
        z_own(a, dst, k, slot, p, target).wait_send()
        z_side(a, dst, k, slot, p, target).wait_send()

    def up_k(p):
        return (1, kz.at[p], 0, 0, p, 1)

    def up_v(p):
        return (2, vz.at[p], 1, 1, p, 1)

    def down_two(p):
        return (0, qz.at[0, p], 0, 2, p, 1)

    def down_three(p):
        return (0, qz.at[1, p], 0, 3, p, 1)

    def down_near(p):
        return (0, qz.at[0, p], 1, 2, p, 2)

    lent = [2 * j for j in range(quarter)]
    order = []
    for j in range(pairs // 4):
        order += [pairs // 2 + j, j]
    order += list(range(pairs // 4, pairs // 2))

    def pair_of(u):
        return order[u] + quarter * x if u in lent else order[u]

    def loan_of(j):
        return pairs // 2 + j + quarter * (1 - x)

    def w_of(r, q):
        return wall.at[r, :, q]

    def y_copy(u):
        return remote(w_ref.at[:, pair_of(u)], w_of(me_dp, pair_of(u)), y_send.at[u], y_recv.at[u], dp=across)

    def lend(j):
        q = pair_of(lent[j])
        return remote(w_of(across, q), w_of(across, q), wx_send.at[j], wx_recv.at[j], sp=side)

    def borrowed(j):
        q = loan_of(j)
        return remote(w_of(across, q), w_of(across, q), wx_send.at[j], wx_recv.at[j], sp=side)

    def forward(q):
        return remote(w_of(across, q), w_of(across, q), f_send.at[q], f_recv.at[q], dp=partner)

    p_copy = remote(w_ref, wall.at[me_dp], p_send, p_recv, dp=partner)
    w_own = pltpu.make_async_copy(w_ref, wall.at[me_dp], w_sem)

    g_copy.start()
    g_own.start()

    @pl.when(z < 2)
    def _():
        for p in range(pairs):
            for a in (1, 2, 0):
                x_copy(a, p).start()

    @pl.when(z >= 2)
    def _():
        for p in range(pairs):
            x_copy(0, p).start()
        for p in range(pairs):
            for a in (1, 2):
                x_copy(a, p).start()

    ahead = min(2, pairs)

    @pl.when(z == 0)
    def _():
        for p in range(ahead):
            z_own(*up_k(p)).start()
            z_own(*up_v(p)).start()

    @pl.when(z == 2)
    def _():
        for p in range(ahead):
            z_own(*down_two(p)).start()

    @pl.when(z == 3)
    def _():
        for p in range(ahead):
            z_own(*down_three(p)).start()
            z_own(*down_near(p)).start()

    for u in range(units):
        y_copy(u).start()
    for p in range(pairs):
        for a in range(3):
            x_own(a, p).start()
    p_copy.start()
    w_own.start()

    def pass_on(u):
        y_copy(u).wait_recv()
        if u in lent:
            lend(lent.index(u)).start()
        forward(pair_of(u)).start()

    def pass_loan(j):
        borrowed(j).wait_recv()
        forward(loan_of(j)).start()

    def arrived(a, p):
        x_own(a, p).wait()
        x_copy(a, p).wait_recv()

    def part_copies(k, slot, p, target):
        return (
            remote(part_o.at[k, p], got_o.at[slot, p], po_send.at[k, p], po_recv.at[slot, p], sp=target * 2 + x),
            remote(part_l.at[k, p], got_l.at[slot, p], pl_send.at[k, p], pl_recv.at[slot, p], sp=target * 2 + x),
        )

    def o_copy(p):
        return remote(ob.at[p, rows_of(1 - x), :], att.at[p, :, half_of(x)], o_send.at[p], o_recv.at[p], sp=side)

    def gates_of(block, p):
        return jnp.concatenate([gb[2 * block, p], gb[2 * block + 1, p]], axis=1)

    def finish(p, value):
        ob[p] = value.astype(jnp.bfloat16)
        o_copy(p).start()
        att[p, :, half_of(x)] = ob[p, rows_of(x), :]

    def share(p, k, slot, target, value, lse):
        part_o[k, p] = value.astype(jnp.bfloat16)
        turned = jnp.transpose(lse)
        part_l[k, p] = jnp.concatenate([turned[0:1], turned[HEAD_DIM:HEAD_DIM + 1]], axis=0)
        for copy in part_copies(k, slot, p, target):
            copy.start()

    def join(p, slots):
        outs, sums = [held_o[p]], [held_l[p]]
        for slot in slots:
            for copy in part_copies(0, slot, p, 0):
                copy.wait_recv()
            outs.append(got_o[slot, p].astype(jnp.float32))
            lse = got_l[slot, p]
            sums.append(jnp.transpose(jnp.concatenate(
                [jnp.broadcast_to(lse[h:h + 1], (HEAD_DIM, 2 * L)) for h in range(2)], axis=0)))
        peak = functools.reduce(jnp.maximum, sums)
        scale = [jnp.exp(s - peak) for s in sums]
        finish(p, sum(o * s for o, s in zip(outs, scale)) / sum(scale))

    def each(body, begin=0, end=None):
        def step(p, carry):
            body(p)
            return carry
        lax.fori_loop(begin, pairs if end is None else end, step, 0)

    def gates_here():
        g_own.wait()
        g_copy.wait_recv()

    def gates_up(target):
        return remote(gb.at[pl.ds(0, 2)], gb.at[pl.ds(0, 2)], g_send.at[1], g_recv.at[2], sp=target * 2 + x)

    def passing(p, first, every):
        for u in range(units):
            at = first + every * u
            if at < pairs:
                @pl.when(p == at)
                def _(u=u):
                    pass_on(u)

    def passed(first, every):
        return [u for u in range(units) if first + every * u < pairs]

    def pass_rest(first, every):
        for u in range(len(passed(first, every)), units):
            pass_on(u)

    def push(p, makers):
        @pl.when(p + ahead < pairs)
        def _():
            for make in makers:
                z_own(*make(p + ahead)).start()
        for make in makers:
            if make in (up_v, up_k):
                arrived(make(p)[0], p)
            z_side(*make(p)).start()

    @pl.when(z == 0)
    def _():
        gates_here()
        gates_up(1).start()
        def work(p):
            push(p, (up_k, up_v))
            arrived(0, p)
            finish(p, attend_rows(qx[p], [(kx[p], vx[p], gates_of(0, p))], True)[0])
            passing(p, 3, 3)
        each(work)
        pass_rest(3, 3)

    @pl.when(z == 1)
    def _():
        gates_here()
        gates_up(0).wait_recv()
        def work(p):
            arrived(1, p)
            arrived(2, p)
            z_arrived(1, kz.at[p], 0, p)
            z_arrived(2, vz.at[p], 1, p)
            lower = (kz[p], vz[p], gates_of(0, p))
            own = (kx[p], vx[p], gates_of(1, p))
            for k in (1, 0):
                z_arrived(0, qz.at[k, p], 2 + k, p)
                share(p, k, 0, 2 + k, *attend_rows(qz[k, p], [lower, own], False))
            arrived(0, p)
            finish(p, attend_rows(qx[p], [lower, own], True)[0])
            passing(p, 1, 2)
        each(work)
        pass_rest(1, 2)

    @pl.when(z == 2)
    def _():
        def pushes(p):
            arrived(0, p)
            push(p, (down_two,))
        each(pushes)
        gates_here()
        lag = min(2, pairs)
        def work(p):
            arrived(1, p)
            arrived(2, p)
            own = (kx[p], vx[p], gates_of(2, p))
            z_arrived(0, qz.at[0, p], 2, p)
            share(p, 1, 1, 3, *attend_rows(qz[0, p], [own], False))
            held_o[p], held_l[p] = attend_rows(qx[p], [own], True)
            @pl.when(p >= lag)
            def _():
                join(p - lag, (0,))
            passing(p, 1, 2)
        each(work)
        each(lambda p: join(p, (0,)), pairs - lag)
        pass_rest(1, 2)

    @pl.when(z == 3)
    def _():
        def pushes(p):
            arrived(0, p)
            push(p, (down_three, down_near))
        each(pushes)
        gates_here()
        def work(p):
            arrived(1, p)
            arrived(2, p)
            held_o[p], held_l[p] = attend_rows(qx[p], [(kx[p], vx[p], gates_of(3, p))], True)
            passing(p, 1, 4)
        each(work)
        def last(p):
            join(p, (0, 1))
            for u in range(len(passed(1, 4)), units):
                @pl.when(p == 2 * (u - len(passed(1, 4))))
                def _(u=u):
                    pass_on(u)
        each(last)

    for j in range(quarter):
        pass_loan(j)

    w_own.wait()
    p_copy.wait_recv()
    steps = [0, 1, 4, 2, 5, 6, 3, 7] if pairs == 8 else list(range(pairs))
    for at, q in enumerate(steps):
        o_copy(q).wait_recv()
        forward(q).wait_recv()
        left = att[q]
        for r in range(ndp):
            columns = slice(r * w_cols, (r + 1) * w_cols)
            part = jnp.dot(left, wall[r, :, q].reshape(2 * LANES, w_cols), preferred_element_type=jnp.float32)
            if at > 0:
                part = acc[:, columns] + part
            if at < pairs - 1:
                acc[:, columns] = part
            else:
                o_ref[:, columns] = part.astype(o_ref.dtype)

    p_copy.wait_send()
    g_copy.wait_send()

    @pl.when(z == 0)
    def _():
        def left(p):
            z_sent(*up_k(p))
            z_sent(*up_v(p))
        each(left)
        gates_up(1).wait_send()

    @pl.when(z == 1)
    def _():
        def left(p):
            for k in range(2):
                for copy in part_copies(k, 0, p, 2 + k):
                    copy.wait_send()
        each(left)

    @pl.when(z == 2)
    def _():
        def left(p):
            z_sent(*down_two(p))
            for copy in part_copies(1, 1, p, 3):
                copy.wait_send()
        each(left)

    @pl.when(z == 3)
    def _():
        def left(p):
            z_sent(*down_three(p))
            z_sent(*down_near(p))
        each(left)

    def sent(p):
        o_copy(p).wait_send()
        forward(p).wait_send()
        for a in range(3):
            x_copy(a, p).wait_send()
    each(sent)
    for u in range(units):
        y_copy(u).wait_send()
    for j in range(quarter):
        lend(j).wait_send()


def fused(n, ndp, queries, keys, values, gate_totals, w_out):
    L, model = queries.shape[1], queries.shape[2]
    heads = gate_totals.shape[2] // 2
    pairs = heads * HEAD_DIM // LANES
    gates = jnp.transpose(gate_totals[0]).reshape(2, pairs, 2, L)
    w_cols = w_out.shape[1]
    weights = w_out.reshape(2, pairs, LANES, w_cols)
    bf16, f32 = jnp.bfloat16, jnp.float32
    dma = pltpu.SemaphoreType.DMA
    block = (pairs, 2 * L, LANES)
    units, quarter = 3 * pairs // 4, pairs // 4
    out = pl.pallas_call(
        functools.partial(kernel, n, ndp),
        out_shape=jax.ShapeDtypeStruct((L, w_cols * ndp), bf16),
        in_specs=[pl.BlockSpec(memory_space=pl.ANY)] * 5,
        out_specs=pl.BlockSpec(memory_space=pltpu.VMEM),
        scratch_shapes=[
            *[pltpu.VMEM(block, bf16)] * 5,
            pltpu.VMEM((2,) + block, bf16),
            pltpu.VMEM((n, pairs, 2, L), f32),
            pltpu.VMEM(block, bf16),
            pltpu.VMEM(block, f32),
            pltpu.VMEM(block, f32),
            pltpu.VMEM((2,) + block, bf16),
            pltpu.VMEM((2, pairs, 2, 2 * L), f32),
            pltpu.VMEM((2,) + block, bf16),
            pltpu.VMEM((2, pairs, 2, 2 * L), f32),
            pltpu.VMEM((pairs, L, 2 * LANES), bf16),
            pltpu.VMEM((ndp, 2, pairs, LANES, w_cols), bf16),
            pltpu.VMEM((L, ndp * w_cols), f32),
            dma((3, pairs)), dma((3, pairs)), dma((2,)), dma((3,)), dma((3, pairs)), dma,
            dma((2, 2, pairs)), dma((4, 2, pairs)),
            dma((2, pairs)), dma((2, pairs)), dma((2, pairs)), dma((2, pairs)),
            dma((pairs,)), dma((pairs,)),
            dma((units,)), dma((units,)), dma((quarter,)), dma((quarter,)), dma, dma,
            dma((pairs,)), dma((pairs,)),
        ],
        compiler_params=pltpu.CompilerParams(
            collective_id=0, has_side_effects=True, vmem_limit_bytes=67043328),
        name="fused_attention",
    )(queries[0], keys[0], values[0], gates, weights)
    return out[None]


def solution(mesh):
    n, ndp = mesh.shape["sp"], mesh.shape["dp"]

    def local(queries, keys, values, gate_totals, w_out):
        fits = n == 8 and ndp == 4 and queries.shape[1] % LANES == 0 and queries.shape[2] % (8 * LANES) == 0
        if fits:
            return fused(n, ndp, queries, keys, values, gate_totals, w_out)
        return general(queries, keys, values, gate_totals, w_out)

    placed = (P("dp", "sp", None),) * 4 + (P(None, "dp"),)
    return jax.shard_map(
        local, mesh=mesh, in_specs=placed, out_specs=P("dp", "sp", None), check_vma=False)
```

```python
import functools

import jax
import jax.numpy as jnp
from jax import lax
from jax.experimental import pallas as pl
from jax.experimental.pallas import tpu as pltpu
from jax.sharding import PartitionSpec as P

HEAD_DIM = 64
LANES = 128
W_CHUNKS = 16
MESH = pl.DeviceIdType.MESH


def attend(queries, key_rows, value_rows, totals):
    length = queries.shape[0]
    block_rows = min(length, 512)
    pieces = []
    for begin_row in range(0, length, block_rows):
        end_row = begin_row + block_rows
        scaled = queries[begin_row:end_row] * jnp.bfloat16(HEAD_DIM ** (-0.5))
        scores = jnp.einsum(
            "qhd,khd->hqk", scaled, key_rows[:end_row], preferred_element_type=jnp.float32
        )
        causal = jnp.arange(end_row)[None, :] <= (begin_row + jnp.arange(block_rows))[:, None]
        scores = jnp.where(
            causal[None],
            scores
            + jnp.transpose(totals[begin_row:end_row])[:, :, None]
            - jnp.transpose(totals[:end_row])[:, None, :],
            -jnp.inf,
        )
        biggest = jnp.max(scores, axis=-1, keepdims=True)
        expo = jnp.exp(scores - biggest)
        summed = jnp.sum(expo, axis=-1)
        weights = expo.astype(jnp.bfloat16)
        output = jnp.einsum(
            "hqk,khd->qhd", weights, value_rows[:end_row], preferred_element_type=jnp.float32
        )
        output = output / jnp.transpose(summed)[:, :, None]
        pieces.append(output.astype(jnp.bfloat16))
    return jnp.concatenate(pieces, axis=0).reshape(length, -1)


def general(queries, keys, values, gate_totals, w_out):
    moved = [
        lax.all_to_all(x, "sp", split_axis=2, concat_axis=1, tiled=True)
        for x in (queries, keys, values, gate_totals)
    ]
    length = moved[0].shape[1]
    heads = [x[0].reshape(length, -1, HEAD_DIM) for x in moved[:3]]
    attended = attend(heads[0], heads[1], heads[2], moved[3][0])[None]
    rows = lax.all_to_all(attended, "sp", split_axis=1, concat_axis=2, tiled=True)
    mixed = jnp.dot(
        rows[0],
        lax.all_gather(w_out, "dp", axis=1, tiled=True),
        preferred_element_type=jnp.float32,
    )
    return mixed.astype(jnp.bfloat16)[None]


def attend_rows(queries, parts, diagonal):
    rows = queries.shape[0]
    scaled = queries * jnp.bfloat16(HEAD_DIM ** -0.5)
    lane = lax.broadcasted_iota(jnp.int32, (rows, LANES), 1)
    outs, sums = [], []
    for h in range(2):
        mine = (lane < HEAD_DIM) if h == 0 else (lane >= HEAD_DIM)
        scores = []
        for at, (keys, _, gates) in enumerate(parts):
            head_keys = jnp.where(mine, keys, jnp.zeros_like(keys))
            score = lax.dot_general(
                scaled, head_keys, (((1,), (1,)), ((), ())), preferred_element_type=jnp.float32)
            score = score - gates[h:h + 1, :]
            if diagonal and at == len(parts) - 1:
                causal = lax.broadcasted_iota(jnp.int32, score.shape, 1) <= lax.broadcasted_iota(
                    jnp.int32, score.shape, 0)
                score = jnp.where(causal, score, -jnp.inf)
            scores.append(score)
        peak = functools.reduce(jnp.maximum, [jnp.max(x, axis=1, keepdims=True) for x in scores])
        expo = [jnp.exp(x - peak) for x in scores]
        total = sum(jnp.sum(x, axis=1, keepdims=True) for x in expo)
        out = sum(
            jnp.dot(x.astype(jnp.bfloat16), part[1], preferred_element_type=jnp.float32)
            for x, part in zip(expo, parts))
        outs.append(out / total)
        sums.append(peak + jnp.log(total))
    first = lane < HEAD_DIM
    return jnp.where(first, outs[0], outs[1]), jnp.where(first, sums[0], sums[1])


def kernel(n, ndp, q_ref, k_ref, v_ref, g_ref, w_ref, o_ref,
           qx, kvx, zin, gb, ob, held_o, held_l, part_o, part_l, got_o, got_l, att, wall, acc,
           q_recv, kv_recv, x_send, g_send, g_recv, z_send, z_recv, po_send, po_recv, pl_send, pl_recv,
           o_send, o_recv, y_recv, yh_recv, wx_recv, wz_recv, w_recv, w_send):
    me = lax.axis_index("sp")
    x = lax.rem(me, 2)
    z = lax.div(me, 2)
    side = me + 1 - 2 * x
    me_dp = lax.axis_index("dp")
    core = lax.rem(me_dp, 2)
    row_y = lax.div(me_dp, 2)
    across = (1 - row_y) * 2 + core
    partner = row_y * 2 + 1 - core
    L = q_ref.shape[0]
    pairs = qx.shape[0]
    W = pairs * LANES
    w_cols = w_ref.shape[3]
    quarter = pairs // 4
    units = quarter * 2
    step_z = quarter // 2
    odd = lax.rem(z, 2)
    other_z = z + 1 - 2 * odd

    barrier = pltpu.get_barrier_semaphore()
    meets = {0: (1,), 1: (0, 2, 3), 2: (1, 3), 3: (1, 2)}
    for here, others in meets.items():
        @pl.when(z == here)
        def _(others=others):
            for other in others:
                pl.semaphore_signal(barrier, inc=1, device_id={"sp": other * 2 + x}, device_id_type=MESH)
    pl.semaphore_signal(barrier, inc=1, device_id={"sp": side}, device_id_type=MESH)
    for other in (partner, across):
        pl.semaphore_signal(barrier, inc=1, device_id={"dp": other}, device_id_type=MESH)
    for here, others in meets.items():
        @pl.when(z == here)
        def _(others=others):
            pl.semaphore_wait(barrier, len(others) + 3)

    def remote(src, dst, send, recv, **device):
        return pltpu.make_async_remote_copy(
            src_ref=src, dst_ref=dst, send_sem=send, recv_sem=recv, device_id=device, device_id_type=MESH)

    def rows_of(which):
        return pl.ds(pl.multiple_of(which * L, L), L)

    def lanes_of(which, p):
        return pl.ds(pl.multiple_of(which * W + p * LANES, LANES), LANES)

    def half_of(which):
        return pl.ds(pl.multiple_of(which * LANES, LANES), LANES)

    def landing(a, p):
        return qx.at[p] if a == 0 else kvx.at[p, a - 1]

    refs = (q_ref, k_ref, v_ref)

    def x_sem(a, p):
        return q_recv.at[p] if a == 0 else kv_recv.at[p]

    def x_copy(a, p):
        return remote(refs[a].at[:, lanes_of(1 - x, p)], landing(a, p).at[rows_of(x), :], x_send, x_sem(a, p), sp=side)

    def x_own(a, p):
        return pltpu.make_async_copy(refs[a].at[:, lanes_of(x, p)], landing(a, p).at[rows_of(x), :], x_sem(a, p))

    def landed(ref, sem):
        remote(ref, ref, x_send, sem, sp=side).wait_recv()

    def left(ref, sem):
        remote(ref, ref, sem, w_recv.at[0], sp=side).wait_send()

    def queries_here(p):
        landed(qx.at[p], q_recv.at[p])

    def keys_here(p):
        landed(kvx.at[p], kv_recv.at[p])

    g_copy = remote(g_ref.at[1 - x], gb.at[me], g_send.at[0], g_recv.at[0], sp=side)
    g_own = pltpu.make_async_copy(g_ref.at[x], gb.at[me], g_recv.at[1])

    def z_own(a, slot, target, p):
        return remote(refs[a].at[:, lanes_of(x, p)], zin.at[p, slot, rows_of(x), :],
                      z_send, z_recv.at[p], sp=target * 2 + x)

    def z_side(a, slot, target, p):
        return remote(landing(a, p).at[rows_of(1 - x), :], zin.at[p, slot, rows_of(1 - x), :],
                      z_send, z_recv.at[p], sp=target * 2 + x)

    up = ((1, 0, 1), (2, 1, 1))
    down_two = ((0, 2, 1),)
    down_three = ((0, 3, 1), (0, 2, 2))

    def sided(j, other):
        which = 1 - x if other else x
        return pairs // 2 + j + quarter * which

    def neighboured(j, other):
        which = 1 - odd if other else odd
        return quarter + j + step_z * which

    def w_of(r, q):
        return wall.at[r, :, q]

    def y_pair(u):
        return sided(u, False) if u < quarter else u - quarter

    def y_copy(u):
        return remote(w_ref.at[:, y_pair(u)], w_of(me_dp, y_pair(u)), w_send, y_recv.at[u], dp=across)

    def y_half(j, h):
        q = neighboured(j, False)
        return remote(w_ref.at[h, q], wall.at[me_dp, h, q], w_send, yh_recv.at[j, h], dp=across)

    def y_last(other=False):
        q = sided(quarter - 1, True)
        return remote(w_ref.at[1, q], wall.at[me_dp, 1, q], w_send, yh_recv.at[step_z, 0], dp=across)

    def side_copy(j, other=False):
        q = sided(j, other)
        ref = wall.at[across, 0, q] if j == quarter - 1 else w_of(across, q)
        return remote(ref, ref, w_send, wx_recv.at[j], sp=side)

    def near_copy(j, h, other=False):
        q = neighboured(j, other)
        return remote(wall.at[across, h, q], wall.at[across, h, q], w_send, wz_recv.at[j, h],
                      sp=other_z * 2 + x)

    def forward(q):
        return remote(w_of(across, q), w_of(across, q), w_send, w_recv.at[q], dp=partner)

    def p_copy(q):
        return remote(w_ref.at[:, q], w_of(me_dp, q), w_send, w_recv.at[q], dp=partner)

    def w_own(q):
        return pltpu.make_async_copy(w_ref.at[:, q], w_of(me_dp, q), w_recv.at[q])

    ahead = min(2, pairs)

    def lead(makers):
        for p in range(ahead):
            for make in makers:
                z_own(*make, p).start()

    def gates_out():
        g_copy.start()
        g_own.start()

    @pl.when(z == 0)
    def _():
        for p in range(pairs):
            for a in (1, 2):
                x_copy(a, p).start()
            if p == 0:
                gates_out()
                lead(up)
        for p in range(pairs):
            x_copy(0, p).start()

    @pl.when(z == 1)
    def _():
        for p in range(pairs):
            for a in (1, 2, 0):
                x_copy(a, p).start()
            if p == 0:
                gates_out()

    @pl.when(z >= 2)
    def _():
        for p in range(pairs):
            x_copy(0, p).start()
            if p == 0:
                @pl.when(z == 2)
                def _():
                    lead(down_two)

                @pl.when(z == 3)
                def _():
                    lead(down_three)
        gates_out()
        for p in range(pairs):
            for a in (1, 2):
                x_copy(a, p).start()

    for j in range(step_z):
        for h in range(2):
            y_half(j, h).start()
    for u in range(units):
        y_copy(u).start()
    y_last().start()
    for p in range(pairs):
        for a in range(3):
            x_own(a, p).start()

    def pass_on(u):
        y_copy(u).wait_recv()
        if u < quarter:
            side_copy(u).start()
        forward(y_pair(u)).start()

    def pass_loan(j):
        side_copy(j, True).wait_recv()
        if j == quarter - 1:
            y_last().wait_recv()
        forward(sided(j, True)).start()

    def near_here(h):
        for j in range(step_z):
            y_half(j, h).wait_recv()
            if h == 1:
                forward(neighboured(j, False)).start()

    def near_lend(h):
        for j in range(step_z):
            near_copy(j, h).start()

    def near_loan():
        for j in range(step_z):
            for h in range(2):
                near_copy(j, h, True).wait_recv()
            forward(neighboured(j, True)).start()

    def share_weights(p):
        p_copy(p).start()
        w_own(p).start()

    def part_copies(k, slot, p, target):
        return (
            remote(part_o.at[k, p], got_o.at[p, slot], po_send, po_recv.at[p], sp=target * 2 + x),
            remote(part_l.at[k, p], got_l.at[p, slot], pl_send, pl_recv.at[p], sp=target * 2 + x),
        )

    def o_copy(p):
        return remote(ob.at[p, rows_of(1 - x), :], att.at[p, :, half_of(x)], o_send, o_recv.at[p], sp=side)

    def gates_of(block, p):
        return jnp.concatenate([gb[2 * block, p], gb[2 * block + 1, p]], axis=1)

    def finish(p, value):
        ob[p] = value.astype(jnp.bfloat16)
        o_copy(p).start()
        att[p, :, half_of(x)] = ob[p, rows_of(x), :]

    def share(p, k, slot, target, value, lse):
        part_o[k, p] = value.astype(jnp.bfloat16)
        turned = jnp.transpose(lse)
        part_l[k, p] = jnp.concatenate([turned[0:1], turned[HEAD_DIM:HEAD_DIM + 1]], axis=0)
        for copy in part_copies(k, slot, p, target):
            copy.start()

    def join(p, slots):
        outs, sums = [held_o[p]], [held_l[p]]
        landed(got_o.at[p] if len(slots) == 2 else got_o.at[p, 0], po_recv.at[p])
        landed(got_l.at[p] if len(slots) == 2 else got_l.at[p, 0], pl_recv.at[p])
        for slot in slots:
            outs.append(got_o[p, slot].astype(jnp.float32))
            lse = got_l[p, slot]
            sums.append(jnp.transpose(jnp.concatenate(
                [jnp.broadcast_to(lse[h:h + 1], (HEAD_DIM, 2 * L)) for h in range(2)], axis=0)))
        peak = functools.reduce(jnp.maximum, sums)
        scale = [jnp.exp(s - peak) for s in sums]
        finish(p, sum(o * s for o, s in zip(outs, scale)) / sum(scale))

    def each(body, begin=0, end=None):
        def step(p, carry):
            body(p)
            return carry
        lax.fori_loop(begin, pairs if end is None else end, step, 0)

    def gates_here():
        g_own.wait()
        g_copy.wait_recv()

    def gates_up(target):
        return remote(gb.at[pl.ds(0, 2)], gb.at[pl.ds(0, 2)], g_send.at[1], g_recv.at[2], sp=target * 2 + x)

    def passing(p, table):
        for at, calls in table.items():
            @pl.when(p == at)
            def _(calls=calls):
                for call in calls:
                    call()

    def on(u):
        return lambda: pass_on(u)

    def near_all():
        near_here(0)
        near_here(1)

    def near_lend_all():
        near_lend(0)
        near_lend(1)

    def push(p, makers):
        for make in makers:
            z_side(*make, p).start()
        @pl.when(p + ahead < pairs)
        def _():
            for make in makers:
                z_own(*make, p + ahead).start()

    @pl.when(z == 0)
    def _():
        def pushes(p):
            keys_here(p)
            push(p, up)
            @pl.when(p == 0)
            def _():
                gates_here()
                gates_up(1).start()
        each(pushes)
        def work(p):
            queries_here(p)
            finish(p, attend_rows(qx[p], [(kvx[p, 0], kvx[p, 1], gates_of(0, p))], True)[0])
            share_weights(p)
            passing(p, {0: [near_all], 3: [on(0)], 7: [on(1)]})
        each(work)
        near_lend_all()
        near_loan()
        pass_on(2)

    @pl.when(z == 1)
    def _():
        gates_here()
        gates_up(0).wait_recv()
        def work(p):
            keys_here(p)
            landed(zin.at[p], z_recv.at[p])
            lower = (zin[p, 0], zin[p, 1], gates_of(0, p))
            own = (kvx[p, 0], kvx[p, 1], gates_of(1, p))
            for k in (1, 0):
                share(p, k, 0, 2 + k, *attend_rows(zin[p, 2 + k], [lower, own], False))
            queries_here(p)
            finish(p, attend_rows(qx[p], [lower, own], True)[0])
            share_weights(p)
            passing(p, {0: [near_all, near_lend_all], 1: [on(0)], 3: [on(1)], 5: [on(2)]})
        each(work)

    @pl.when(z == 2)
    def _():
        def pushes(p):
            queries_here(p)
            push(p, down_two)
            passing(p, {2: [lambda: near_here(0), lambda: near_lend(0)], 6: [lambda: near_here(1), lambda: near_lend(1)]})
        each(pushes)
        gates_here()
        lag = min(2, pairs)
        def work(p):
            keys_here(p)
            own = (kvx[p, 0], kvx[p, 1], gates_of(2, p))
            landed(zin.at[p, 2], z_recv.at[p])
            share(p, 1, 1, 3, *attend_rows(zin[p, 2], [own], False))
            held_o[p], held_l[p] = attend_rows(qx[p], [own], True)
            @pl.when(p >= lag)
            def _():
                join(p - lag, (0,))
            share_weights(p)
            passing(p, {2: [on(0)], 4: [on(1)], 6: [on(2)]})
        each(work)
        each(lambda p: join(p, (0,)), pairs - lag)

    @pl.when(z == 3)
    def _():
        def pushes(p):
            queries_here(p)
            push(p, down_three)
        each(pushes)
        gates_here()
        def work(p):
            keys_here(p)
            held_o[p], held_l[p] = attend_rows(qx[p], [(kvx[p, 0], kvx[p, 1], gates_of(3, p))], True)
            share_weights(p)
            passing(p, {0: [near_all, near_lend_all], 2: [near_loan], 4: [on(0)], 7: [on(1)]})
        each(work)
        def last(p):
            join(p, (0, 1))
            passing(p, {4: [on(2)]})
        each(last)

    for u in range(3, units):
        pass_on(u)
    pass_loan(0)

    @pl.when((z == 1) | (z == 2))
    def _():
        near_loan()

    for j in range(1, quarter):
        pass_loan(j)

    for at, q in enumerate(range(pairs)):
        landed(wall.at[pl.ds(0, 3), :, q], w_recv.at[q])
        o_copy(q).wait_recv()
        lhs = att[q]
        for r in range(ndp):
            columns = slice(r * w_cols, (r + 1) * w_cols)
            part = jnp.dot(lhs, wall[r, :, q].reshape(2 * LANES, w_cols), preferred_element_type=jnp.float32)
            if at > 0:
                part = acc[:, columns] + part
            if at < pairs - 1:
                acc[:, columns] = part
            else:
                o_ref[:, columns] = part.astype(o_ref.dtype)

    g_copy.wait_send()

    @pl.when(z == 0)
    def _():
        left(wall.at[0, 0], z_send)
        gates_up(1).wait_send()

    @pl.when(z == 1)
    def _():
        left(part_o, po_send)
        left(part_l, pl_send)

    @pl.when(z == 2)
    def _():
        left(wall.at[0, 0, pl.ds(0, pairs // 2)], z_send)
        left(part_o.at[1], po_send)
        left(part_l.at[1], pl_send)

    @pl.when(z == 3)
    def _():
        left(wall.at[0, 0], z_send)

    left(ob.at[:, pl.ds(0, L), :], o_send)
    left(wall.at[0, 0, pl.ds(0, 3 * pairs // 4)], x_send)
    left(wall.at[pl.ds(0, 3)], w_send)


def fused(n, ndp, queries, keys, values, gate_totals, w_out):
    L, model = queries.shape[1], queries.shape[2]
    heads = gate_totals.shape[2] // 2
    pairs = heads * HEAD_DIM // LANES
    gates = jnp.transpose(gate_totals[0]).reshape(2, pairs, 2, L)
    w_cols = w_out.shape[1]
    weights = w_out.reshape(2, pairs, LANES, w_cols)
    bf16, f32 = jnp.bfloat16, jnp.float32
    dma = pltpu.SemaphoreType.DMA
    block = (pairs, 2 * L, LANES)
    quarter = pairs // 4
    units, step_z = 2 * quarter, quarter // 2
    out = pl.pallas_call(
        functools.partial(kernel, n, ndp),
        out_shape=jax.ShapeDtypeStruct((L, w_cols * ndp), bf16),
        in_specs=[pl.BlockSpec(memory_space=pltpu.HBM)] * 5,
        out_specs=pl.BlockSpec(memory_space=pltpu.VMEM),
        scratch_shapes=[
            pltpu.VMEM(block, bf16),
            pltpu.VMEM((pairs, 2) + block[1:], bf16),
            pltpu.VMEM((pairs, 4) + block[1:], bf16),
            pltpu.VMEM((n, pairs, 2, L), f32),
            pltpu.VMEM(block, bf16),
            pltpu.VMEM(block, f32),
            pltpu.VMEM(block, f32),
            pltpu.VMEM((2,) + block, bf16),
            pltpu.VMEM((2, pairs, 2, 2 * L), f32),
            pltpu.VMEM((pairs, 2) + block[1:], bf16),
            pltpu.VMEM((pairs, 2, 2, 2 * L), f32),
            pltpu.VMEM((pairs, L, 2 * LANES), bf16),
            pltpu.VMEM((ndp, 2, pairs, LANES, w_cols), bf16),
            pltpu.VMEM((L, ndp * w_cols), f32),
            dma((pairs,)), dma((pairs,)), dma, dma((2,)), dma((3,)), dma, dma((pairs,)),
            dma, dma((pairs,)), dma, dma((pairs,)),
            dma, dma((pairs,)), dma((units,)), dma((step_z + 1, 2)), dma((quarter,)), dma((step_z, 2)),
            dma((pairs,)), dma,
        ],
        compiler_params=pltpu.CompilerParams(
            collective_id=0, has_side_effects=True, vmem_limit_bytes=48 * 2**20),
        name="fused_attention",
    )(*[pltpu.with_memory_space_constraint(t, pltpu.HBM) for t in (queries[0], keys[0], values[0], gates, weights)])
    return out[None]


def solution(mesh):
    n, ndp = mesh.shape["sp"], mesh.shape["dp"]

    def local(queries, keys, values, gate_totals, w_out):
        fits = n == 8 and ndp == 4 and queries.shape[1] % LANES == 0 and queries.shape[2] == 2 * n * LANES
        if fits:
            return fused(n, ndp, queries, keys, values, gate_totals, w_out)
        return general(queries, keys, values, gate_totals, w_out)

    placed = (P("dp", "sp", None),) * 4 + (P(None, "dp"),)
    return jax.shard_map(
        local, mesh=mesh, in_specs=placed, out_specs=P("dp", "sp", None), check_vma=False)
```

```python
import functools

import jax
import jax.numpy as jnp
from jax import lax
from jax.experimental import pallas as pl
from jax.experimental.pallas import tpu as pltpu
from jax.sharding import PartitionSpec as P

HEAD_DIM = 64
LANES = 128
LOG2E = 1.4426950408889634
MESH = pl.DeviceIdType.MESH


def attend(queries, key_rows, value_rows, totals):
    length = queries.shape[0]
    block_rows = min(length, 512)
    pieces = []
    for begin_row in range(0, length, block_rows):
        end_row = begin_row + block_rows
        scaled = queries[begin_row:end_row] * jnp.bfloat16(HEAD_DIM ** (-0.5))
        scores = jnp.einsum(
            "qhd,khd->hqk", scaled, key_rows[:end_row], preferred_element_type=jnp.float32
        )
        causal = jnp.arange(end_row)[None, :] <= (begin_row + jnp.arange(block_rows))[:, None]
        scores = jnp.where(
            causal[None],
            scores
            + jnp.transpose(totals[begin_row:end_row])[:, :, None]
            - jnp.transpose(totals[:end_row])[:, None, :],
            -jnp.inf,
        )
        biggest = jnp.max(scores, axis=-1, keepdims=True)
        expo = jnp.exp(scores - biggest)
        summed = jnp.sum(expo, axis=-1)
        weights = expo.astype(jnp.bfloat16)
        output = jnp.einsum(
            "hqk,khd->qhd", weights, value_rows[:end_row], preferred_element_type=jnp.float32
        )
        output = output / jnp.transpose(summed)[:, :, None]
        pieces.append(output.astype(jnp.bfloat16))
    return jnp.concatenate(pieces, axis=0).reshape(length, -1)


def general(queries, keys, values, gate_totals, w_out):
    moved = [
        lax.all_to_all(x, "sp", split_axis=2, concat_axis=1, tiled=True)
        for x in (queries, keys, values, gate_totals)
    ]
    length = moved[0].shape[1]
    heads = [x[0].reshape(length, -1, HEAD_DIM) for x in moved[:3]]
    attended = attend(heads[0], heads[1], heads[2], moved[3][0])[None]
    rows = lax.all_to_all(attended, "sp", split_axis=1, concat_axis=2, tiled=True)
    mixed = jnp.dot(
        rows[0],
        lax.all_gather(w_out, "dp", axis=1, tiled=True),
        preferred_element_type=jnp.float32,
    )
    return mixed.astype(jnp.bfloat16)[None]


def attend_rows(tasks, parts):
    def of_head(h, array, other):
        lane = lax.broadcasted_iota(jnp.int32, array.shape, 1)
        return jnp.where((lane < HEAD_DIM) if h == 0 else (lane >= HEAD_DIM), array, jnp.full_like(array, other))

    chains = [(i, h) for i in range(len(tasks)) for h in range(2)]
    scaled = [queries * jnp.bfloat16(HEAD_DIM ** -0.5) for queries, _ in tasks]
    head_keys = [[of_head(h, part[0], 0) for part in parts] for h in range(2)]
    head_values = [[of_head(h, part[1], 1) for part in parts] for h in range(2)]
    gates = [part[2] * LOG2E for part in parts]
    scores, peaks, weights, sums = {}, {}, {}, {}
    for i, h in chains:
        scores[i, h] = [
            lax.dot_general(scaled[i], keys, (((1,), (1,)), ((), ())), preferred_element_type=jnp.float32)
            for keys in head_keys[h]]
    for i, h in chains:
        rows = [score * LOG2E - gate[h:h + 1, :] for score, gate in zip(scores[i, h], gates)]
        if tasks[i][1]:
            shape = rows[-1].shape
            causal = lax.broadcasted_iota(jnp.int32, shape, 1) <= lax.broadcasted_iota(jnp.int32, shape, 0)
            rows[-1] = jnp.where(causal, rows[-1], -jnp.inf)
        scores[i, h] = rows
        peaks[i, h] = functools.reduce(jnp.maximum, [jnp.max(x, axis=1, keepdims=True) for x in rows])
    for i, h in chains:
        weights[i, h] = [jnp.exp2(x - peaks[i, h]).astype(jnp.bfloat16) for x in scores[i, h]]
    for i, h in chains:
        sums[i, h] = sum(
            jnp.dot(x, values, preferred_element_type=jnp.float32)
            for x, values in zip(weights[i, h], head_values[h]))
    results = []
    for i in range(len(tasks)):
        first = lax.broadcasted_iota(jnp.int32, sums[i, 0].shape, 1) < HEAD_DIM
        out = jnp.where(first, sums[i, 0], sums[i, 1])
        total = pltpu.roll(jnp.where(first, sums[i, 1], sums[i, 0]), HEAD_DIM, 1)
        results.append((out / total, jnp.where(first, peaks[i, 0], peaks[i, 1]) + jnp.log2(total)))
    return results


def kernel(n, ndp, q_ref, k_ref, v_ref, g_ref, w_ref, o_ref,
           qx, kvx, zin, gb, ob, held_o, held_l, near_o, near_l, part_o, part_l, got_o, got_l, att, wall, acc,
           q_recv, kv_recv, x_send, g_send, g_recv, z_send, z_recv, po_send, po_recv, pl_send, pl_recv,
           o_send, o_recv, y_recv, yh_recv, wx_recv, wz_recv, w_recv, w_send):
    me = lax.axis_index("sp")
    x = lax.rem(me, 2)
    z = lax.div(me, 2)
    side = me + 1 - 2 * x
    me_dp = lax.axis_index("dp")
    core = lax.rem(me_dp, 2)
    row_y = lax.div(me_dp, 2)
    across = (1 - row_y) * 2 + core
    partner = row_y * 2 + 1 - core
    L = q_ref.shape[0]
    pairs = qx.shape[0]
    W = pairs * LANES
    w_cols = w_ref.shape[3]
    quarter = pairs // 4
    units = quarter * 2
    step_z = quarter // 2
    odd = lax.rem(z, 2)
    other_z = z + 1 - 2 * odd

    barrier = pltpu.get_barrier_semaphore()
    meets = {0: (1,), 1: (0, 2, 3), 2: (1, 3), 3: (1, 2)}
    for here, others in meets.items():
        @pl.when(z == here)
        def _(others=others):
            for other in others:
                pl.semaphore_signal(barrier, inc=1, device_id={"sp": other * 2 + x}, device_id_type=MESH)
    pl.semaphore_signal(barrier, inc=1, device_id={"sp": side}, device_id_type=MESH)
    for other in (partner, across):
        pl.semaphore_signal(barrier, inc=1, device_id={"dp": other}, device_id_type=MESH)
    for here, others in meets.items():
        @pl.when(z == here)
        def _(others=others):
            pl.semaphore_wait(barrier, len(others) + 3)

    def remote(src, dst, send, recv, **device):
        return pltpu.make_async_remote_copy(
            src_ref=src, dst_ref=dst, send_sem=send, recv_sem=recv, device_id=device, device_id_type=MESH)

    def rows_of(which):
        return pl.ds(pl.multiple_of(which * L, L), L)

    def lanes_of(which, p):
        return pl.ds(pl.multiple_of(which * W + p * LANES, LANES), LANES)

    def half_of(which):
        return pl.ds(pl.multiple_of(which * LANES, LANES), LANES)

    def landing(a, p):
        return qx.at[p] if a == 0 else kvx.at[p, a - 1]

    refs = (q_ref, k_ref, v_ref)

    def x_sem(a, p):
        return q_recv.at[p] if a == 0 else kv_recv.at[p]

    def x_copy(a, p):
        return remote(refs[a].at[:, lanes_of(1 - x, p)], landing(a, p).at[rows_of(x), :], x_send, x_sem(a, p), sp=side)

    def x_own(a, p):
        return pltpu.make_async_copy(refs[a].at[:, lanes_of(x, p)], landing(a, p).at[rows_of(x), :], x_sem(a, p))

    def landed(ref, sem):
        remote(ref, ref, x_send, sem, sp=side).wait_recv()

    def left(ref, sem):
        remote(ref, ref, sem, w_recv.at[0], sp=side).wait_send()

    def queries_here(p):
        landed(qx.at[p], q_recv.at[p])

    def keys_here(p):
        landed(kvx.at[p], kv_recv.at[p])

    g_copy = remote(g_ref.at[1 - x], gb.at[me], g_send.at[0], g_recv.at[0], sp=side)
    g_own = pltpu.make_async_copy(g_ref.at[x], gb.at[me], g_recv.at[1])

    def z_own(a, slot, target, p):
        return remote(refs[a].at[:, lanes_of(x, p)], zin.at[p, slot, rows_of(x), :],
                      z_send, z_recv.at[p], sp=target * 2 + x)

    def z_side(a, slot, target, p):
        return remote(landing(a, p).at[rows_of(1 - x), :], zin.at[p, slot, rows_of(1 - x), :],
                      z_send, z_recv.at[p], sp=target * 2 + x)

    up = ((1, 0, 1), (2, 1, 1))
    down_two = ((0, 2, 1),)

    def sided(j, other):
        which = 1 - x if other else x
        return pairs // 2 + j + quarter * which

    def neighboured(j, other):
        which = 1 - odd if other else odd
        return quarter + j + step_z * which

    def w_of(r, q):
        return wall.at[r, :, q]

    def y_pair(u):
        return sided(u, False) if u < quarter else u - quarter

    def y_copy(u):
        return remote(w_ref.at[:, y_pair(u)], w_of(me_dp, y_pair(u)), w_send, y_recv.at[u], dp=across)

    def y_half(j, h):
        q = neighboured(j, False)
        return remote(w_ref.at[h, q], wall.at[me_dp, h, q], w_send, yh_recv.at[j, h], dp=across)

    def y_last(other=False):
        q = sided(quarter - 1, True)
        return remote(w_ref.at[1, q], wall.at[me_dp, 1, q], w_send, yh_recv.at[step_z, 0], dp=across)

    def side_copy(j, other=False):
        q = sided(j, other)
        ref = wall.at[across, 0, q] if j == quarter - 1 else w_of(across, q)
        return remote(ref, ref, w_send, wx_recv.at[j], sp=side)

    def near_copy(j, h, other=False):
        q = neighboured(j, other)
        return remote(wall.at[across, h, q], wall.at[across, h, q], w_send, wz_recv.at[j, h],
                      sp=other_z * 2 + x)

    def forward(q):
        return remote(w_of(across, q), w_of(across, q), w_send, w_recv.at[q], dp=partner)

    def p_copy(q):
        return remote(w_ref.at[:, q], w_of(me_dp, q), w_send, w_recv.at[q], dp=partner)

    def w_own(q):
        return pltpu.make_async_copy(w_ref.at[:, q], w_of(me_dp, q), w_recv.at[q])

    direct = pairs - 2
    ahead = min(3, pairs)

    def lead(makers):
        for p in range(ahead):
            for make in makers:
                z_own(*make, p).start()

    def gates_out():
        g_copy.start()
        g_own.start()

    @pl.when(z == 0)
    def _():
        for p in range(pairs):
            for a in (1, 2):
                x_copy(a, p).start()
            if p == 0:
                gates_out()
                lead(up)
        for p in range(pairs):
            x_copy(0, p).start()

    @pl.when(z == 1)
    def _():
        for p in range(pairs):
            for a in (1, 2, 0):
                x_copy(a, p).start()
            if p == 0:
                gates_out()

    @pl.when(z == 2)
    def _():
        for p in range(ahead):
            x_copy(0, p).start()
            if p == 0:
                lead(down_two)
            if p + direct < pairs:
                x_copy(0, p + direct).start()
        gates_out()
        for i in range(pairs):
            for a in (1, 2):
                x_copy(a, (i + direct) % pairs).start()
            if i + ahead < direct:
                x_copy(0, i + ahead).start()

    @pl.when(z == 3)
    def _():
        for p in range(direct):
            x_copy(0, p).start()
            if p + direct < pairs:
                x_copy(0, p + direct).start()
            if p == 0:
                for i in range(ahead):
                    z_own(0, 3, 1, i).start()
                    z_own(0, 2, 2, (i + direct) % pairs).start()
        gates_out()
        for p in range(pairs):
            for a in (1, 2):
                x_copy(a, p).start()

    for j in range(step_z):
        for h in range(2):
            y_half(j, h).start()
    for u in range(units):
        y_copy(u).start()
    y_last().start()
    for p in range(pairs):
        for a in range(3):
            x_own(a, p).start()

    def pass_on(u):
        y_copy(u).wait_recv()
        if u < quarter:
            side_copy(u).start()
        forward(y_pair(u)).start()

    def pass_loan(j):
        side_copy(j, True).wait_recv()
        if j == quarter - 1:
            y_last().wait_recv()
        forward(sided(j, True)).start()

    def near_here(h):
        for j in range(step_z):
            y_half(j, h).wait_recv()
            if h == 1:
                forward(neighboured(j, False)).start()

    def near_lend(h):
        for j in range(step_z):
            near_copy(j, h).start()

    def near_loan():
        for j in range(step_z):
            for h in range(2):
                near_copy(j, h, True).wait_recv()
            forward(neighboured(j, True)).start()

    def share_weights(p):
        p_copy(p).start()
        w_own(p).start()

    def part_copies(k, slot, p, target):
        return (
            remote(part_o.at[k, p], got_o.at[p, slot], po_send, po_recv.at[p], sp=target * 2 + x),
            remote(part_l.at[k, p], got_l.at[p, slot], pl_send, pl_recv.at[p], sp=target * 2 + x),
        )

    def o_copy(p):
        return remote(ob.at[p, rows_of(1 - x), :], att.at[p, :, half_of(x)], o_send, o_recv.at[p], sp=side)

    def gates_of(block, p):
        return jnp.concatenate([gb[2 * block, p], gb[2 * block + 1, p]], axis=1)

    def finish(p, value):
        ob[p] = value.astype(jnp.bfloat16)
        o_copy(p).start()
        att[p, :, half_of(x)] = ob[p, rows_of(x), :]

    def send_part(p, k, slot, target):
        for copy in part_copies(k, slot, p, target):
            copy.start()

    def share(p, k, slot, target, value, lse):
        store_part(p, k, value, lse)
        send_part(p, k, slot, target)

    def store_part(p, k, value, lse):
        part_o[k, p] = value.astype(jnp.bfloat16)
        turned = jnp.transpose(lse)
        part_l[k, p] = jnp.concatenate([turned[0:1], turned[HEAD_DIM:HEAD_DIM + 1]], axis=0)

    def merged(p, o_ref, l_ref, slots):
        outs, sums = [o_ref[p]], [l_ref[p]]
        for slot in slots:
            outs.append(got_o[p, slot].astype(jnp.float32))
            lse = got_l[p, slot]
            sums.append(jnp.transpose(jnp.concatenate(
                [jnp.broadcast_to(lse[h:h + 1], (HEAD_DIM, 2 * L)) for h in range(2)], axis=0)))
        peak = functools.reduce(jnp.maximum, sums)
        scale = [jnp.exp2(s - peak) for s in sums]
        total = sum(scale)
        return sum(o * s for o, s in zip(outs, scale)) / total, peak + jnp.log2(total)

    def parts_here(p, slots):
        landed(got_o.at[p] if len(slots) == 2 else got_o.at[p, slots[0]], po_recv.at[p])
        landed(got_l.at[p] if len(slots) == 2 else got_l.at[p, slots[0]], pl_recv.at[p])

    def join(p, slots):
        parts_here(p, slots)
        finish(p, merged(p, held_o, held_l, slots)[0])

    def join_two(p):
        @pl.when(p < direct)
        def _():
            parts_here(p, (0, 1))
            share(p, 1, 1, 3, *merged(p, near_o, near_l, (1,)))
            finish(p, merged(p, held_o, held_l, (0,))[0])

        @pl.when(p >= direct)
        def _():
            join(p, (0,))

    def join_three(p):
        @pl.when(p < direct)
        def _():
            join(p, (1,))

        @pl.when(p >= direct)
        def _():
            join(p, (0, 1))

    def each(body, begin=0, end=None):
        def step(p, carry):
            body(p)
            return carry
        lax.fori_loop(begin, pairs if end is None else end, step, 0)

    def gates_here():
        g_own.wait()
        g_copy.wait_recv()

    def gates_up(target):
        return remote(gb.at[pl.ds(0, 2)], gb.at[pl.ds(0, 2)], g_send.at[1], g_recv.at[2], sp=target * 2 + x)

    def passing(p, table):
        for at, calls in table.items():
            @pl.when(p == at)
            def _(calls=calls):
                for call in calls:
                    call()

    def on(u):
        return lambda: pass_on(u)

    def near_all():
        near_here(0)
        near_here(1)

    def near_lend_all():
        near_lend(0)
        near_lend(1)

    def push(p, makers):
        for make in makers:
            z_side(*make, p).start()
        @pl.when(p + ahead < pairs)
        def _():
            for make in makers:
                z_own(*make, p + ahead).start()

    @pl.when(z == 0)
    def _():
        def pushes(p):
            keys_here(p)
            push(p, up)
            @pl.when(p == 0)
            def _():
                gates_here()
                gates_up(1).start()
        each(pushes)
        def work(p):
            queries_here(p)
            finish(p, attend_rows([(qx[p], True)], [(kvx[p, 0], kvx[p, 1], gates_of(0, p))])[0][0])
            share_weights(p)
            passing(p, {0: [near_all], 3: [on(0)], 7: [on(1)]})
        each(work)
        near_lend_all()
        near_loan()
        pass_on(2)

    @pl.when(z == 1)
    def _():
        gates_here()
        gates_up(0).wait_recv()
        def work(p):
            keys_here(p)
            landed(zin.at[p], z_recv.at[p])
            lower = (zin[p, 0], zin[p, 1], gates_of(0, p))
            own = (kvx[p, 0], kvx[p, 1], gates_of(1, p))
            queries_here(p)
            three, two, one = attend_rows([(zin[p, 3], False), (zin[p, 2], False), (qx[p], True)], [lower, own])
            store_part(p, 1, *three)
            @pl.when(p < direct)
            def _():
                send_part(p, 1, 1, 2)

            @pl.when(p >= direct)
            def _():
                send_part(p, 1, 0, 3)
            share(p, 0, 0, 2, *two)
            finish(p, one[0])
            share_weights(p)
            passing(p, {0: [near_all, near_lend_all], 2: [on(0)], 4: [on(1)], 6: [on(2)]})
        each(work)

    @pl.when(z == 2)
    def _():
        for p in range(ahead):
            queries_here(p)
            push(p, down_two)
            if p + direct < pairs:
                queries_here(p + direct)
        near_here(0)
        near_lend(0)
        gates_here()
        lag = pairs - direct
        def work(i):
            p = lax.rem(i + direct, pairs)
            keys_here(p)
            own = (kvx[p, 0], kvx[p, 1], gates_of(2, p))
            landed(zin.at[p, 2], z_recv.at[p])
            three, (held_o[p], held_l[p]) = attend_rows([(zin[p, 2], False), (qx[p], True)], [own])
            near_o[p], near_l[p] = three
            @pl.when(p >= direct)
            def _():
                share(p, 1, 1, 3, near_o[p], near_l[p])
            @pl.when(i + ahead < pairs)
            def _():
                @pl.when(i + ahead < direct)
                def _():
                    queries_here(i + ahead)
                push(i + ahead, down_two)
            passing(i, {0: [lambda: near_here(1), lambda: near_lend(1)], 3: [on(0)], 5: [on(1)]})
            @pl.when(i >= lag)
            def _():
                join_two(i - lag)
            share_weights(p)
            passing(i, {pairs - 1: [on(2)]})
        each(work)
        def last(p):
            join_two(p)
            passing(p, {pairs - 2: [lambda: pass_loan(0), on(3)]})
        each(last, direct)

    @pl.when(z == 3)
    def _():
        for i in range(pairs):
            if i < direct:
                queries_here(i)
            if i + direct < pairs:
                queries_here(i + direct)
            near = (i + direct) % pairs
            z_side(0, 3, 1, i).start()
            z_side(0, 2, 2, near).start()
            if i + ahead < pairs:
                z_own(0, 3, 1, i + ahead).start()
                z_own(0, 2, 2, (near + ahead) % pairs).start()
        gates_here()
        def work(p):
            keys_here(p)
            held_o[p], held_l[p] = attend_rows([(qx[p], True)], [(kvx[p, 0], kvx[p, 1], gates_of(3, p))])[0]
            share_weights(p)
            passing(p, {0: [near_all, near_lend_all], 4: [on(0)], 7: [near_loan, on(1)]})
        each(work)
        def last(p):
            join_three(p)
            passing(p, {3: [on(2)], 4: [lambda: pass_loan(0)], 6: [on(3)]})
        each(last)

    @pl.when(z == 0)
    def _():
        pass_loan(0)
        pass_on(3)

    @pl.when(z == 1)
    def _():
        pass_loan(0)
        near_loan()
        pass_on(3)

    @pl.when(z == 2)
    def _():
        near_loan()

    @pl.when(z >= 2)
    def _():
        pass_loan(1)

    early = list(range(pairs - 3)) + [pairs - 3 + x]
    steps = early + [pairs - 2 - x, pairs - 1]
    for at, q in enumerate(steps):
        if at == len(early):
            @pl.when(z < 2)
            def _():
                pass_loan(1)
        landed(wall.at[pl.ds(0, 3), :, q], w_recv.at[q])
        o_copy(q).wait_recv()
        lhs = att[q]
        for r in range(ndp):
            columns = slice(r * w_cols, (r + 1) * w_cols)
            part = jnp.dot(lhs, wall[r, :, q].reshape(2 * LANES, w_cols), preferred_element_type=jnp.float32)
            if at > 0:
                part = acc[:, columns] + part
            if at < pairs - 1:
                acc[:, columns] = part
            else:
                o_ref[:, columns] = part.astype(o_ref.dtype)

    g_copy.wait_send()

    @pl.when(z == 0)
    def _():
        left(wall.at[0, 0], z_send)
        gates_up(1).wait_send()

    @pl.when(z == 1)
    def _():
        left(part_o, po_send)
        left(part_l, pl_send)

    @pl.when(z == 2)
    def _():
        left(wall.at[0, 0, pl.ds(0, pairs // 2)], z_send)
        left(part_o.at[1], po_send)
        left(part_l.at[1], pl_send)

    @pl.when(z == 3)
    def _():
        left(wall.at[0, 0], z_send)

    left(ob.at[:, pl.ds(0, L), :], o_send)
    left(wall.at[0, 0, pl.ds(0, 3 * pairs // 4)], x_send)
    left(wall.at[pl.ds(0, 3)], w_send)


def fused(n, ndp, queries, keys, values, gate_totals, w_out):
    L, model = queries.shape[1], queries.shape[2]
    heads = gate_totals.shape[2] // 2
    pairs = heads * HEAD_DIM // LANES
    gates = jnp.transpose(gate_totals[0]).reshape(2, pairs, 2, L)
    w_cols = w_out.shape[1]
    weights = w_out.reshape(2, pairs, LANES, w_cols)
    bf16, f32 = jnp.bfloat16, jnp.float32
    dma = pltpu.SemaphoreType.DMA
    block = (pairs, 2 * L, LANES)
    quarter = pairs // 4
    units, step_z = 2 * quarter, quarter // 2
    out = pl.pallas_call(
        functools.partial(kernel, n, ndp),
        out_shape=jax.ShapeDtypeStruct((L, w_cols * ndp), bf16),
        in_specs=[pl.BlockSpec(memory_space=pltpu.HBM)] * 5,
        out_specs=pl.BlockSpec(memory_space=pltpu.VMEM),
        scratch_shapes=[
            pltpu.VMEM(block, bf16),
            pltpu.VMEM((pairs, 2) + block[1:], bf16),
            pltpu.VMEM((pairs, 4) + block[1:], bf16),
            pltpu.VMEM((n, pairs, 2, L), f32),
            pltpu.VMEM(block, bf16),
            *[pltpu.VMEM(block, f32)] * 4,
            pltpu.VMEM((2,) + block, bf16),
            pltpu.VMEM((2, pairs, 2, 2 * L), f32),
            pltpu.VMEM((pairs, 2) + block[1:], bf16),
            pltpu.VMEM((pairs, 2, 2, 2 * L), f32),
            pltpu.VMEM((pairs, L, 2 * LANES), bf16),
            pltpu.VMEM((ndp, 2, pairs, LANES, w_cols), bf16),
            pltpu.VMEM((L, ndp * w_cols), f32),
            dma((pairs,)), dma((pairs,)), dma, dma((2,)), dma((3,)), dma, dma((pairs,)),
            dma, dma((pairs,)), dma, dma((pairs,)),
            dma, dma((pairs,)), dma((units,)), dma((step_z + 1, 2)), dma((quarter,)), dma((step_z, 2)),
            dma((pairs,)), dma,
        ],
        compiler_params=pltpu.CompilerParams(
            collective_id=0, has_side_effects=True, vmem_limit_bytes=48 * 2**20),
        name="fused_attention",
    )(*[pltpu.with_memory_space_constraint(t, pltpu.HBM) for t in (queries[0], keys[0], values[0], gates, weights)])
    return out[None]


def solution(mesh):
    n, ndp = mesh.shape["sp"], mesh.shape["dp"]

    def local(queries, keys, values, gate_totals, w_out):
        fits = n == 8 and ndp == 4 and queries.shape[1] % LANES == 0 and queries.shape[2] == 2 * n * LANES
        if fits:
            return fused(n, ndp, queries, keys, values, gate_totals, w_out)
        return general(queries, keys, values, gate_totals, w_out)

    placed = (P("dp", "sp", None),) * 4 + (P(None, "dp"),)
    return jax.shard_map(
        local, mesh=mesh, in_specs=placed, out_specs=P("dp", "sp", None), check_vma=False)
```

```python
import functools

import jax
import jax.numpy as jnp
from jax import lax
from jax.experimental import pallas as pl
from jax.experimental.pallas import tpu as pltpu
from jax.sharding import PartitionSpec as P

HEAD_DIM = 64
LANES = 128
LOG2E = 1.4426950408889634
MESH = pl.DeviceIdType.MESH


def attend(queries, key_rows, value_rows, totals):
    length = queries.shape[0]
    block_rows = min(length, 512)
    pieces = []
    for begin_row in range(0, length, block_rows):
        end_row = begin_row + block_rows
        scaled = queries[begin_row:end_row] * jnp.bfloat16(HEAD_DIM ** (-0.5))
        scores = jnp.einsum(
            "qhd,khd->hqk", scaled, key_rows[:end_row], preferred_element_type=jnp.float32
        )
        causal = jnp.arange(end_row)[None, :] <= (begin_row + jnp.arange(block_rows))[:, None]
        scores = jnp.where(
            causal[None],
            scores
            + jnp.transpose(totals[begin_row:end_row])[:, :, None]
            - jnp.transpose(totals[:end_row])[:, None, :],
            -jnp.inf,
        )
        biggest = jnp.max(scores, axis=-1, keepdims=True)
        expo = jnp.exp(scores - biggest)
        summed = jnp.sum(expo, axis=-1)
        weights = expo.astype(jnp.bfloat16)
        output = jnp.einsum(
            "hqk,khd->qhd", weights, value_rows[:end_row], preferred_element_type=jnp.float32
        )
        output = output / jnp.transpose(summed)[:, :, None]
        pieces.append(output.astype(jnp.bfloat16))
    return jnp.concatenate(pieces, axis=0).reshape(length, -1)


def general(queries, keys, values, gate_totals, w_out):
    moved = [
        lax.all_to_all(x, "sp", split_axis=2, concat_axis=1, tiled=True)
        for x in (queries, keys, values, gate_totals)
    ]
    length = moved[0].shape[1]
    heads = [x[0].reshape(length, -1, HEAD_DIM) for x in moved[:3]]
    attended = attend(heads[0], heads[1], heads[2], moved[3][0])[None]
    rows = lax.all_to_all(attended, "sp", split_axis=1, concat_axis=2, tiled=True)
    mixed = jnp.dot(
        rows[0],
        lax.all_gather(w_out, "dp", axis=1, tiled=True),
        preferred_element_type=jnp.float32,
    )
    return mixed.astype(jnp.bfloat16)[None]


def attend_rows(tasks, parts):
    def of_head(h, array, other):
        lane = lax.broadcasted_iota(jnp.int32, array.shape, 1)
        return jnp.where((lane < HEAD_DIM) if h == 0 else (lane >= HEAD_DIM), array, jnp.full_like(array, other))

    chains = [(i, h) for i in range(len(tasks)) for h in range(2)]
    scaled = [queries * jnp.bfloat16(HEAD_DIM ** -0.5) for queries, _ in tasks]
    head_keys = [[of_head(h, part[0], 0) for part in parts] for h in range(2)]
    head_values = [[of_head(h, part[1], 1) for part in parts] for h in range(2)]
    gates = [part[2] * LOG2E for part in parts]
    scores, peaks, weights, sums = {}, {}, {}, {}
    for i, h in chains:
        scores[i, h] = [
            lax.dot_general(scaled[i], keys, (((1,), (1,)), ((), ())), preferred_element_type=jnp.float32)
            for keys in head_keys[h]]
    for i, h in chains:
        rows = [score * LOG2E - gate[h:h + 1, :] for score, gate in zip(scores[i, h], gates)]
        if tasks[i][1]:
            shape = rows[-1].shape
            causal = lax.broadcasted_iota(jnp.int32, shape, 1) <= lax.broadcasted_iota(jnp.int32, shape, 0)
            rows[-1] = jnp.where(causal, rows[-1], -jnp.inf)
        scores[i, h] = rows
        peaks[i, h] = functools.reduce(jnp.maximum, [jnp.max(x, axis=1, keepdims=True) for x in rows])
    for i, h in chains:
        weights[i, h] = [jnp.exp2(x - peaks[i, h]).astype(jnp.bfloat16) for x in scores[i, h]]
    for i, h in chains:
        sums[i, h] = sum(
            jnp.dot(x, values, preferred_element_type=jnp.float32)
            for x, values in zip(weights[i, h], head_values[h]))
    results = []
    for i in range(len(tasks)):
        first = lax.broadcasted_iota(jnp.int32, sums[i, 0].shape, 1) < HEAD_DIM
        out = jnp.where(first, sums[i, 0], sums[i, 1])
        total = pltpu.roll(jnp.where(first, sums[i, 1], sums[i, 0]), HEAD_DIM, 1)
        results.append((out / total, jnp.where(first, peaks[i, 0], peaks[i, 1]) + jnp.log2(total)))
    return results


def kernel(n, ndp, q_ref, k_ref, v_ref, g_ref, w_ref, o_ref,
           qx, kvx, zin, gb, ob, held_o, held_l, near_o, near_l, part_o, part_l, got_o, got_l, tail_o, tail_l, att, wall, acc,
           q_recv, kv_recv, x_send, g_send, g_recv, z_send, z_recv, po_send, po_recv, pl_send, pl_recv,
           o_send, o_recv, t_recv, y_recv, yh_recv, wx_recv, wz_recv, w_recv, w_send):
    me = lax.axis_index("sp")
    x = lax.rem(me, 2)
    z = lax.div(me, 2)
    side = me + 1 - 2 * x
    me_dp = lax.axis_index("dp")
    core = lax.rem(me_dp, 2)
    row_y = lax.div(me_dp, 2)
    across = (1 - row_y) * 2 + core
    partner = row_y * 2 + 1 - core
    L = q_ref.shape[0]
    pairs = qx.shape[0]
    W = pairs * LANES
    w_cols = w_ref.shape[3]
    quarter = pairs // 4
    units = quarter * 2
    step_z = quarter // 2
    odd = lax.rem(z, 2)
    other_z = z + 1 - 2 * odd

    barrier = pltpu.get_barrier_semaphore()
    meets = {0: (1,), 1: (0, 2, 3), 2: (1, 3), 3: (1, 2)}
    for here, others in meets.items():
        @pl.when(z == here)
        def _(others=others):
            for other in others:
                pl.semaphore_signal(barrier, inc=1, device_id={"sp": other * 2 + x}, device_id_type=MESH)
    pl.semaphore_signal(barrier, inc=1, device_id={"sp": side}, device_id_type=MESH)
    for other in (partner, across):
        pl.semaphore_signal(barrier, inc=1, device_id={"dp": other}, device_id_type=MESH)
    for here, others in meets.items():
        @pl.when(z == here)
        def _(others=others):
            pl.semaphore_wait(barrier, len(others) + 3)

    def remote(src, dst, send, recv, **device):
        return pltpu.make_async_remote_copy(
            src_ref=src, dst_ref=dst, send_sem=send, recv_sem=recv, device_id=device, device_id_type=MESH)

    def rows_of(which):
        return pl.ds(pl.multiple_of(which * L, L), L)

    def lanes_of(which, p):
        return pl.ds(pl.multiple_of(which * W + p * LANES, LANES), LANES)

    def half_of(which):
        return pl.ds(pl.multiple_of(which * LANES, LANES), LANES)

    def landing(a, p):
        return qx.at[p] if a == 0 else kvx.at[p, a - 1]

    refs = (q_ref, k_ref, v_ref)

    def x_sem(a, p):
        return q_recv.at[p] if a == 0 else kv_recv.at[p]

    def x_copy(a, p):
        return remote(refs[a].at[:, lanes_of(1 - x, p)], landing(a, p).at[rows_of(x), :], x_send, x_sem(a, p), sp=side)

    def x_own(a, p):
        return pltpu.make_async_copy(refs[a].at[:, lanes_of(x, p)], landing(a, p).at[rows_of(x), :], x_sem(a, p))

    def landed(ref, sem):
        remote(ref, ref, x_send, sem, sp=side).wait_recv()

    def left(ref, sem):
        remote(ref, ref, sem, w_recv.at[0], sp=side).wait_send()

    def queries_here(p):
        landed(qx.at[p], q_recv.at[p])

    def keys_here(p):
        landed(kvx.at[p], kv_recv.at[p])

    g_copy = remote(g_ref.at[1 - x], gb.at[me], g_send.at[0], g_recv.at[0], sp=side)
    g_own = pltpu.make_async_copy(g_ref.at[x], gb.at[me], g_recv.at[1])

    def z_own(a, slot, target, p):
        return remote(refs[a].at[:, lanes_of(x, p)], zin.at[p, slot, rows_of(x), :],
                      z_send, z_recv.at[p], sp=target * 2 + x)

    def z_side(a, slot, target, p):
        return remote(landing(a, p).at[rows_of(1 - x), :], zin.at[p, slot, rows_of(1 - x), :],
                      z_send, z_recv.at[p], sp=target * 2 + x)

    up = ((1, 0, 1), (2, 1, 1))
    down_two = ((0, 2, 1),)

    def sided(j, other):
        which = 1 - x if other else x
        return pairs // 2 + j + quarter * which

    def neighboured(j, other):
        which = 1 - odd if other else odd
        return quarter + j + step_z * which

    def w_of(r, q):
        return wall.at[r, :, q]

    def y_pair(u):
        return sided(u, False) if u < quarter else u - quarter

    def y_copy(u):
        return remote(w_ref.at[:, y_pair(u)], w_of(me_dp, y_pair(u)), w_send, y_recv.at[u], dp=across)

    def y_half(j, h):
        q = neighboured(j, False)
        return remote(w_ref.at[h, q], wall.at[me_dp, h, q], w_send, yh_recv.at[j, h], dp=across)

    def y_last(other=False):
        q = sided(quarter - 1, True)
        return remote(w_ref.at[1, q], wall.at[me_dp, 1, q], w_send, yh_recv.at[step_z, 0], dp=across)

    def side_copy(j, other=False):
        q = sided(j, other)
        ref = wall.at[across, 0, q] if j == quarter - 1 else w_of(across, q)
        return remote(ref, ref, w_send, wx_recv.at[j], sp=side)

    def near_copy(j, h, other=False):
        q = neighboured(j, other)
        return remote(wall.at[across, h, q], wall.at[across, h, q], w_send, wz_recv.at[j, h],
                      sp=other_z * 2 + x)

    def forward(q):
        return remote(w_of(across, q), w_of(across, q), w_send, w_recv.at[q], dp=partner)

    def p_copy(q):
        return remote(w_ref.at[:, q], w_of(me_dp, q), w_send, w_recv.at[q], dp=partner)

    def w_own(q):
        return pltpu.make_async_copy(w_ref.at[:, q], w_of(me_dp, q), w_recv.at[q])

    direct = pairs - 3
    ahead = min(3, pairs)

    def lead(makers):
        for p in range(ahead):
            for make in makers:
                z_own(*make, p).start()

    def gates_out():
        g_copy.start()
        g_own.start()

    @pl.when(z == 0)
    def _():
        gates_out()
        lead(up)
        for p in range(pairs):
            for a in (1, 2):
                x_copy(a, p).start()
        for p in range(pairs):
            x_copy(0, p).start()

    @pl.when(z == 1)
    def _():
        gates_out()
        for p in range(pairs):
            for a in (1, 2, 0):
                x_copy(a, p).start()

    @pl.when(z == 2)
    def _():
        for p in range(ahead):
            x_copy(0, p).start()
            if p == 0:
                lead(down_two)
            if p + direct < pairs:
                x_copy(0, p + direct).start()
        gates_out()
        for i in range(pairs):
            for a in (1, 2):
                x_copy(a, (i + direct) % pairs).start()
            if i + ahead < direct:
                x_copy(0, i + ahead).start()

    @pl.when(z == 3)
    def _():
        for p in range(direct):
            x_copy(0, p).start()
            if p + direct < pairs:
                x_copy(0, p + direct).start()
            if p == 0:
                for i in range(ahead):
                    z_own(0, 3, 1, i).start()
                    z_own(0, 2, 2, (i + direct) % pairs).start()
        gates_out()
        for p in range(pairs):
            for a in (1, 2):
                x_copy(a, p).start()

    for j in range(step_z):
        for h in range(2):
            y_half(j, h).start()
    for u in range(units):
        y_copy(u).start()
    y_last().start()
    for p in range(pairs):
        for a in range(3):
            x_own(a, p).start()

    def pass_on(u):
        y_copy(u).wait_recv()
        if u < quarter:
            side_copy(u).start()
        forward(y_pair(u)).start()

    def pass_loan(j):
        side_copy(j, True).wait_recv()
        if j == quarter - 1:
            y_last().wait_recv()
        forward(sided(j, True)).start()

    def near_here(h):
        for j in range(step_z):
            y_half(j, h).wait_recv()
            if h == 1:
                forward(neighboured(j, False)).start()

    def near_lend(h):
        for j in range(step_z):
            near_copy(j, h).start()

    def near_loan():
        for j in range(step_z):
            for h in range(2):
                near_copy(j, h, True).wait_recv()
            forward(neighboured(j, True)).start()

    def share_weights(p):
        p_copy(p).start()
        w_own(p).start()

    def part_copies(k, slot, p, target):
        return (
            remote(part_o.at[k, p], got_o.at[p, slot], po_send, po_recv.at[p], sp=target * 2 + x),
            remote(part_l.at[k, p], got_l.at[p, slot], pl_send, pl_recv.at[p], sp=target * 2 + x),
        )

    def o_copy(p):
        return remote(ob.at[p, rows_of(1 - x), :], att.at[p, :, half_of(x)], o_send, o_recv.at[p], sp=side)

    def gates_of(block, p):
        return jnp.concatenate([gb[2 * block, p], gb[2 * block + 1, p]], axis=1)

    def finish(p, value):
        ob[p] = value.astype(jnp.bfloat16)
        o_copy(p).start()
        att[p, :, half_of(x)] = ob[p, rows_of(x), :]

    final = pairs - 1

    def tail_copies(k, slot, target, row, o_sem, l_sem):
        return (
            remote(part_o.at[k, final, rows_of(row), :], tail_o.at[slot, x], o_sem, t_recv.at[slot, 0],
                   sp=target * 2 + row),
            remote(part_l.at[k, final, :, rows_of(row)], tail_l.at[slot, x], l_sem, t_recv.at[slot, 1],
                   sp=target * 2 + row),
        )

    def send_part(p, k, slot, target):
        @pl.when(p < final)
        def _():
            for copy in part_copies(k, slot, p, target):
                copy.start()

        @pl.when(p == final)
        def _():
            for row in (1 - x, x):
                for copy in tail_copies(k, slot, target, row, po_send, pl_send):
                    copy.start()

    def hold(p, value, lse):
        @pl.when(p < final)
        def _():
            held_o[p], held_l[p] = value, lse

        @pl.when(p == final)
        def _():
            store_part(final, 0, value, lse)
            for copy in tail_copies(0, 2, z, 1 - x, o_send, g_send.at[1]):
                copy.start()
            tail_o[2, pl.ds(x, 1)] = part_o[0, final, rows_of(x), :][None]
            tail_l[2, pl.ds(x, 1)] = part_l[0, final, :, rows_of(x)][None]

    def join_tail(slots):
        landed(tail_o.at[2, 1 - x], t_recv.at[2, 0])
        landed(tail_l.at[2, 1 - x], t_recv.at[2, 1])
        for slot in slots:
            landed(tail_o.at[slot], t_recv.at[slot, 0])
            landed(tail_l.at[slot], t_recv.at[slot, 1])
        for h in range(2):
            outs, sums = [], []
            for slot in (2,) + slots:
                outs.append(tail_o[slot, h].astype(jnp.float32))
                lse = tail_l[slot, h]
                sums.append(jnp.transpose(jnp.concatenate(
                    [jnp.broadcast_to(lse[j:j + 1], (HEAD_DIM, L)) for j in range(2)], axis=0)))
            peak = functools.reduce(jnp.maximum, sums)
            scale = [jnp.exp2(s - peak) for s in sums]
            value = sum(o * s for o, s in zip(outs, scale)) / sum(scale)
            att[final, :, h * LANES:(h + 1) * LANES] = value.astype(jnp.bfloat16)

    def share(p, k, slot, target, value, lse):
        store_part(p, k, value, lse)
        send_part(p, k, slot, target)

    def store_part(p, k, value, lse):
        part_o[k, p] = value.astype(jnp.bfloat16)
        turned = jnp.transpose(lse)
        part_l[k, p] = jnp.concatenate([turned[0:1], turned[HEAD_DIM:HEAD_DIM + 1]], axis=0)

    def merged(p, o_ref, l_ref, slots):
        outs, sums = [o_ref[p]], [l_ref[p]]
        for slot in slots:
            outs.append(got_o[p, slot].astype(jnp.float32))
            lse = got_l[p, slot]
            sums.append(jnp.transpose(jnp.concatenate(
                [jnp.broadcast_to(lse[h:h + 1], (HEAD_DIM, 2 * L)) for h in range(2)], axis=0)))
        peak = functools.reduce(jnp.maximum, sums)
        scale = [jnp.exp2(s - peak) for s in sums]
        total = sum(scale)
        return sum(o * s for o, s in zip(outs, scale)) / total, peak + jnp.log2(total)

    def parts_here(p, slots):
        landed(got_o.at[p] if len(slots) == 2 else got_o.at[p, slots[0]], po_recv.at[p])
        landed(got_l.at[p] if len(slots) == 2 else got_l.at[p, slots[0]], pl_recv.at[p])

    def join(p, slots):
        parts_here(p, slots)
        finish(p, merged(p, held_o, held_l, slots)[0])

    def join_two(p):
        @pl.when(p < direct)
        def _():
            parts_here(p, (0, 1))
            share(p, 1, 1, 3, *merged(p, near_o, near_l, (1,)))
            finish(p, merged(p, held_o, held_l, (0,))[0])

        @pl.when((p >= direct) & (p < final))
        def _():
            join(p, (0,))

        @pl.when(p == final)
        def _():
            join_tail((0,))

    def join_three(p):
        @pl.when(p < direct)
        def _():
            join(p, (1,))

        @pl.when((p >= direct) & (p < final))
        def _():
            join(p, (0, 1))

        @pl.when(p == final)
        def _():
            join_tail((0, 1))

    def each(body, begin=0, end=None):
        def step(p, carry):
            body(p)
            return carry
        lax.fori_loop(begin, pairs if end is None else end, step, 0)

    def gates_here():
        g_own.wait()
        g_copy.wait_recv()

    def gates_up(target):
        return remote(gb.at[pl.ds(0, 2)], gb.at[pl.ds(0, 2)], g_send.at[1], g_recv.at[2], sp=target * 2 + x)

    def passing(p, table):
        for at, calls in table.items():
            @pl.when(p == at)
            def _(calls=calls):
                for call in calls:
                    call()

    def on(u):
        return lambda: pass_on(u)

    def near_all():
        near_here(0)
        near_here(1)

    def near_lend_all():
        near_lend(0)
        near_lend(1)

    def push(p, makers):
        for make in makers:
            z_side(*make, p).start()
        @pl.when(p + ahead < pairs)
        def _():
            for make in makers:
                z_own(*make, p + ahead).start()

    @pl.when(z == 0)
    def _():
        def pushes(p):
            keys_here(p)
            push(p, up)
        gates_here()
        gates_up(1).start()
        each(pushes)
        def work(p):
            queries_here(p)
            finish(p, attend_rows([(qx[p], True)], [(kvx[p, 0], kvx[p, 1], gates_of(0, p))])[0][0])
            share_weights(p)
            passing(p, {0: [near_all], 3: [on(0)], 7: [on(1)]})
        each(work)
        near_lend_all()
        near_loan()
        pass_on(2)

    @pl.when(z == 1)
    def _():
        gates_here()
        gates_up(0).wait_recv()
        def work(p):
            keys_here(p)
            landed(zin.at[p], z_recv.at[p])
            lower = (zin[p, 0], zin[p, 1], gates_of(0, p))
            own = (kvx[p, 0], kvx[p, 1], gates_of(1, p))
            queries_here(p)
            three, two, one = attend_rows([(zin[p, 3], False), (zin[p, 2], False), (qx[p], True)], [lower, own])
            store_part(p, 1, *three)
            @pl.when(p < direct)
            def _():
                send_part(p, 1, 1, 2)

            @pl.when(p >= direct)
            def _():
                send_part(p, 1, 0, 3)
            share(p, 0, 0, 2, *two)
            finish(p, one[0])
            share_weights(p)
            passing(p, {0: [near_all, near_lend_all], 2: [on(0)], 4: [on(1)], 7: [on(2)]})
        each(work)

    @pl.when(z == 2)
    def _():
        for p in range(ahead):
            queries_here(p)
            push(p, down_two)
            if p + direct < pairs:
                queries_here(p + direct)
        near_here(0)
        near_lend(0)
        gates_here()
        lag = pairs - direct
        def work(i):
            p = lax.rem(i + direct, pairs)
            keys_here(p)
            own = (kvx[p, 0], kvx[p, 1], gates_of(2, p))
            landed(zin.at[p, 2], z_recv.at[p])
            (near_o[p], near_l[p]), mine = attend_rows([(zin[p, 2], False), (qx[p], True)], [own])
            hold(p, *mine)
            @pl.when(p >= direct)
            def _():
                share(p, 1, 1, 3, near_o[p], near_l[p])
            @pl.when(i + ahead < pairs)
            def _():
                @pl.when(i + ahead < direct)
                def _():
                    queries_here(i + ahead)
                push(i + ahead, down_two)
            passing(i, {0: [lambda: near_here(1), lambda: near_lend(1)], 3: [on(0)], 5: [on(1)]})
            @pl.when(i >= lag)
            def _():
                join_two(i - lag)
            share_weights(p)
            passing(i, {pairs - 1: [on(2)]})
        each(work)
        def last(p):
            join_two(p)
            passing(p, {pairs - 2: [lambda: pass_loan(0), near_loan, on(3), lambda: pass_loan(1)]})
        each(last, direct)

    @pl.when(z == 3)
    def _():
        for i in range(pairs):
            if i < direct:
                queries_here(i)
            if i + direct < pairs:
                queries_here(i + direct)
            near = (i + direct) % pairs
            z_side(0, 3, 1, i).start()
            z_side(0, 2, 2, near).start()
            if i + ahead < pairs:
                z_own(0, 3, 1, i + ahead).start()
                z_own(0, 2, 2, (near + ahead) % pairs).start()
        gates_here()
        def work(p):
            keys_here(p)
            hold(p, *attend_rows([(qx[p], True)], [(kvx[p, 0], kvx[p, 1], gates_of(3, p))])[0])
            share_weights(p)
            passing(p, {0: [near_all, near_lend_all], 4: [on(0)], 7: [near_loan, on(1)]})
        each(work)
        def last(p):
            join_three(p)
            passing(p, {3: [on(2)], 4: [lambda: pass_loan(0)], 6: [on(3), lambda: pass_loan(1)]})
        each(last)

    @pl.when(z == 0)
    def _():
        pass_loan(0)
        pass_on(3)
        pass_loan(1)

    @pl.when(z == 1)
    def _():
        pass_loan(0)
        near_loan()
        pass_on(3)
        pass_loan(1)

    for at, q in enumerate(range(pairs)):
        landed(wall.at[pl.ds(0, 3), :, q], w_recv.at[q])
        if at < pairs - 1:
            o_copy(q).wait_recv()
        else:
            @pl.when(z < 2)
            def _():
                o_copy(q).wait_recv()
        lhs = att[q]
        for r in range(ndp):
            columns = slice(r * w_cols, (r + 1) * w_cols)
            part = jnp.dot(lhs, wall[r, :, q].reshape(2 * LANES, w_cols), preferred_element_type=jnp.float32)
            if at > 0:
                part = acc[:, columns] + part
            if at < pairs - 1:
                acc[:, columns] = part
            else:
                o_ref[:, columns] = part.astype(o_ref.dtype)

    g_copy.wait_send()

    @pl.when(z == 0)
    def _():
        left(wall.at[0, 0], z_send)
        gates_up(1).wait_send()

    @pl.when(z == 1)
    def _():
        left(part_o, po_send)
        left(part_l, pl_send)

    @pl.when(z == 2)
    def _():
        left(wall.at[0, 0, pl.ds(0, pairs // 2)], z_send)
        left(part_o.at[1], po_send)
        left(part_l.at[1], pl_send)

    @pl.when(z == 3)
    def _():
        left(wall.at[0, 0], z_send)

    @pl.when(z >= 2)
    def _():
        left(part_l.at[0, final, :, rows_of(1 - x)], g_send.at[1])

    left(ob.at[:, pl.ds(0, L), :], o_send)
    left(wall.at[0, 0, pl.ds(0, 3 * pairs // 4)], x_send)
    left(wall.at[pl.ds(0, 3)], w_send)


def fused(n, ndp, queries, keys, values, gate_totals, w_out):
    L, model = queries.shape[1], queries.shape[2]
    heads = gate_totals.shape[2] // 2
    pairs = heads * HEAD_DIM // LANES
    gates = jnp.transpose(gate_totals[0]).reshape(2, pairs, 2, L)
    w_cols = w_out.shape[1]
    weights = w_out.reshape(2, pairs, LANES, w_cols)
    bf16, f32 = jnp.bfloat16, jnp.float32
    dma = pltpu.SemaphoreType.DMA
    block = (pairs, 2 * L, LANES)
    quarter = pairs // 4
    units, step_z = 2 * quarter, quarter // 2
    out = pl.pallas_call(
        functools.partial(kernel, n, ndp),
        out_shape=jax.ShapeDtypeStruct((L, w_cols * ndp), bf16),
        in_specs=[pl.BlockSpec(memory_space=pltpu.HBM)] * 5,
        out_specs=pl.BlockSpec(memory_space=pltpu.VMEM),
        scratch_shapes=[
            pltpu.VMEM(block, bf16),
            pltpu.VMEM((pairs, 2) + block[1:], bf16),
            pltpu.VMEM((pairs, 4) + block[1:], bf16),
            pltpu.VMEM((n, pairs, 2, L), f32),
            pltpu.VMEM(block, bf16),
            *[pltpu.VMEM(block, f32)] * 4,
            pltpu.VMEM((2,) + block, bf16),
            pltpu.VMEM((2, pairs, 2, 2 * L), f32),
            pltpu.VMEM((pairs, 2) + block[1:], bf16),
            pltpu.VMEM((pairs, 2, 2, 2 * L), f32),
            pltpu.VMEM((3, 2, L, LANES), bf16),
            pltpu.VMEM((3, 2, 2, L), f32),
            pltpu.VMEM((pairs, L, 2 * LANES), bf16),
            pltpu.VMEM((ndp, 2, pairs, LANES, w_cols), bf16),
            pltpu.VMEM((L, ndp * w_cols), f32),
            dma((pairs,)), dma((pairs,)), dma, dma((2,)), dma((3,)), dma, dma((pairs,)),
            dma, dma((pairs,)), dma, dma((pairs,)),
            dma, dma((pairs,)), dma((3, 2)), dma((units,)), dma((step_z + 1, 2)), dma((quarter,)), dma((step_z, 2)),
            dma((pairs,)), dma,
        ],
        compiler_params=pltpu.CompilerParams(
            collective_id=0, has_side_effects=True, vmem_limit_bytes=48 * 2**20),
        name="fused_attention",
    )(*[pltpu.with_memory_space_constraint(t, pltpu.HBM) for t in (queries[0], keys[0], values[0], gates, weights)])
    return out[None]


def solution(mesh):
    n, ndp = mesh.shape["sp"], mesh.shape["dp"]

    def local(queries, keys, values, gate_totals, w_out):
        fits = n == 8 and ndp == 4 and queries.shape[1] % LANES == 0 and queries.shape[2] == 2 * n * LANES
        if fits:
            return fused(n, ndp, queries, keys, values, gate_totals, w_out)
        return general(queries, keys, values, gate_totals, w_out)

    placed = (P("dp", "sp", None),) * 4 + (P(None, "dp"),)
    return jax.shard_map(
        local, mesh=mesh, in_specs=placed, out_specs=P("dp", "sp", None), check_vma=False)
```

```python
import functools

import jax
import jax.numpy as jnp
from jax import lax
from jax.experimental import pallas as pl
from jax.experimental.pallas import tpu as pltpu
from jax.sharding import PartitionSpec as P

HEAD_DIM = 64
LANES = 128
LOG2E = 1.4426950408889634
MESH = pl.DeviceIdType.MESH


def attend(queries, key_rows, value_rows, totals):
    length = queries.shape[0]
    block_rows = min(length, 512)
    pieces = []
    for begin_row in range(0, length, block_rows):
        end_row = begin_row + block_rows
        scaled = queries[begin_row:end_row] * jnp.bfloat16(HEAD_DIM ** (-0.5))
        scores = jnp.einsum(
            "qhd,khd->hqk", scaled, key_rows[:end_row], preferred_element_type=jnp.float32
        )
        causal = jnp.arange(end_row)[None, :] <= (begin_row + jnp.arange(block_rows))[:, None]
        scores = jnp.where(
            causal[None],
            scores
            + jnp.transpose(totals[begin_row:end_row])[:, :, None]
            - jnp.transpose(totals[:end_row])[:, None, :],
            -jnp.inf,
        )
        biggest = jnp.max(scores, axis=-1, keepdims=True)
        expo = jnp.exp(scores - biggest)
        summed = jnp.sum(expo, axis=-1)
        weights = expo.astype(jnp.bfloat16)
        output = jnp.einsum(
            "hqk,khd->qhd", weights, value_rows[:end_row], preferred_element_type=jnp.float32
        )
        output = output / jnp.transpose(summed)[:, :, None]
        pieces.append(output.astype(jnp.bfloat16))
    return jnp.concatenate(pieces, axis=0).reshape(length, -1)


def general(queries, keys, values, gate_totals, w_out):
    moved = [
        lax.all_to_all(x, "sp", split_axis=2, concat_axis=1, tiled=True)
        for x in (queries, keys, values, gate_totals)
    ]
    length = moved[0].shape[1]
    heads = [x[0].reshape(length, -1, HEAD_DIM) for x in moved[:3]]
    attended = attend(heads[0], heads[1], heads[2], moved[3][0])[None]
    rows = lax.all_to_all(attended, "sp", split_axis=1, concat_axis=2, tiled=True)
    mixed = jnp.dot(
        rows[0],
        lax.all_gather(w_out, "dp", axis=1, tiled=True),
        preferred_element_type=jnp.float32,
    )
    return mixed.astype(jnp.bfloat16)[None]


def attend_rows(tasks, parts):
    def of_head(h, array, other):
        lane = lax.broadcasted_iota(jnp.int32, array.shape, 1)
        return jnp.where((lane < HEAD_DIM) if h == 0 else (lane >= HEAD_DIM), array, jnp.full_like(array, other))

    chains = [(i, h) for i in range(len(tasks)) for h in range(2)]
    scaled = [queries * jnp.bfloat16(HEAD_DIM ** -0.5) for queries, _ in tasks]
    head_keys = [[of_head(h, part[0], 0) for part in parts] for h in range(2)]
    head_values = [[of_head(h, part[1], 1) for part in parts] for h in range(2)]
    gates = [part[2] * LOG2E for part in parts]
    scores, peaks, weights, sums = {}, {}, {}, {}
    for i, h in chains:
        scores[i, h] = [
            lax.dot_general(scaled[i], keys, (((1,), (1,)), ((), ())), preferred_element_type=jnp.float32)
            for keys in head_keys[h]]
    for i, h in chains:
        rows = [score * LOG2E - gate[h:h + 1, :] for score, gate in zip(scores[i, h], gates)]
        if tasks[i][1]:
            shape = rows[-1].shape
            causal = lax.broadcasted_iota(jnp.int32, shape, 1) <= lax.broadcasted_iota(jnp.int32, shape, 0)
            rows[-1] = jnp.where(causal, rows[-1], -jnp.inf)
        scores[i, h] = rows
        peaks[i, h] = functools.reduce(jnp.maximum, [jnp.max(x, axis=1, keepdims=True) for x in rows])
    for i, h in chains:
        weights[i, h] = [jnp.exp2(x - peaks[i, h]).astype(jnp.bfloat16) for x in scores[i, h]]
    for i, h in chains:
        sums[i, h] = sum(
            jnp.dot(x, values, preferred_element_type=jnp.float32)
            for x, values in zip(weights[i, h], head_values[h]))
    results = []
    for i in range(len(tasks)):
        first = lax.broadcasted_iota(jnp.int32, sums[i, 0].shape, 1) < HEAD_DIM
        out = jnp.where(first, sums[i, 0], sums[i, 1])
        total = pltpu.roll(jnp.where(first, sums[i, 1], sums[i, 0]), HEAD_DIM, 1)
        results.append((out / total, jnp.where(first, peaks[i, 0], peaks[i, 1]) + jnp.log2(total)))
    return results


def kernel(n, ndp, q_ref, k_ref, v_ref, g_ref, w_ref, o_ref,
           qx, kvx, zin, gb, ob, held_o, held_l, near_o, near_l, part_o, part_l, got_o, got_l, tail_o, tail_l, att, wall, acc,
           q_recv, kv_recv, x_send, g_send, g_recv, z_send, z_recv, po_send, po_recv, pl_send, pl_recv,
           o_send, o_recv, t_recv, y_recv, yh_recv, wx_recv, wz_recv, w_recv, w_send):
    me = lax.axis_index("sp")
    x = lax.rem(me, 2)
    z = lax.div(me, 2)
    side = me + 1 - 2 * x
    me_dp = lax.axis_index("dp")
    core = lax.rem(me_dp, 2)
    row_y = lax.div(me_dp, 2)
    across = (1 - row_y) * 2 + core
    partner = row_y * 2 + 1 - core
    L = q_ref.shape[0]
    pairs = qx.shape[0]
    W = pairs * LANES
    w_cols = w_ref.shape[3]
    quarter = pairs // 4
    units = quarter * 2
    step_z = quarter // 2
    odd = lax.rem(z, 2)
    other_z = z + 1 - 2 * odd

    barrier = pltpu.get_barrier_semaphore()
    meets = {0: (1,), 1: (0, 2, 3), 2: (1, 3), 3: (1, 2)}
    for here, others in meets.items():
        @pl.when(z == here)
        def _(others=others):
            for other in others:
                pl.semaphore_signal(barrier, inc=1, device_id={"sp": other * 2 + x}, device_id_type=MESH)
    pl.semaphore_signal(barrier, inc=1, device_id={"sp": side}, device_id_type=MESH)
    for other in (partner, across):
        pl.semaphore_signal(barrier, inc=1, device_id={"dp": other}, device_id_type=MESH)
    for here, others in meets.items():
        @pl.when(z == here)
        def _(others=others):
            pl.semaphore_wait(barrier, len(others) + 3)

    def remote(src, dst, send, recv, **device):
        return pltpu.make_async_remote_copy(
            src_ref=src, dst_ref=dst, send_sem=send, recv_sem=recv, device_id=device, device_id_type=MESH)

    def rows_of(which):
        return pl.ds(pl.multiple_of(which * L, L), L)

    def lanes_of(which, p):
        return pl.ds(pl.multiple_of(which * W + p * LANES, LANES), LANES)

    def half_of(which):
        return pl.ds(pl.multiple_of(which * LANES, LANES), LANES)

    def landing(a, p):
        return qx.at[p] if a == 0 else kvx.at[p, a - 1]

    refs = (q_ref, k_ref, v_ref)

    def x_sem(a, p):
        return q_recv.at[p] if a == 0 else kv_recv.at[p]

    def x_copy(a, p):
        return remote(refs[a].at[:, lanes_of(1 - x, p)], landing(a, p).at[rows_of(x), :], x_send, x_sem(a, p), sp=side)

    def x_own(a, p):
        return pltpu.make_async_copy(refs[a].at[:, lanes_of(x, p)], landing(a, p).at[rows_of(x), :], x_sem(a, p))

    def landed(ref, sem):
        remote(ref, ref, x_send, sem, sp=side).wait_recv()

    def left(ref, sem):
        remote(ref, ref, sem, w_recv.at[0], sp=side).wait_send()

    def queries_here(p):
        landed(qx.at[p], q_recv.at[p])

    def keys_here(p):
        landed(kvx.at[p], kv_recv.at[p])

    g_copy = remote(g_ref.at[1 - x], gb.at[me], g_send.at[0], g_recv.at[0], sp=side)
    g_own = pltpu.make_async_copy(g_ref.at[x], gb.at[me], g_recv.at[1])

    def z_own(a, slot, target, p):
        return remote(refs[a].at[:, lanes_of(x, p)], zin.at[p, slot, rows_of(x), :],
                      z_send, z_recv.at[p], sp=target * 2 + x)

    def z_side(a, slot, target, p):
        return remote(landing(a, p).at[rows_of(1 - x), :], zin.at[p, slot, rows_of(1 - x), :],
                      z_send, z_recv.at[p], sp=target * 2 + x)

    up = ((1, 0, 1), (2, 1, 1))
    down_two = ((0, 2, 1),)

    def sided(j, other):
        which = 1 - x if other else x
        return pairs // 2 + j + quarter * which

    def neighboured(j, other):
        which = 1 - odd if other else odd
        return quarter + j + step_z * which

    def w_of(r, q):
        return wall.at[r, :, q]

    def y_pair(u):
        return sided(u, False) if u < quarter else u - quarter

    def y_copy(u):
        return remote(w_ref.at[:, y_pair(u)], w_of(me_dp, y_pair(u)), w_send, y_recv.at[u], dp=across)

    def y_half(j, h):
        q = neighboured(j, False)
        return remote(w_ref.at[h, q], wall.at[me_dp, h, q], w_send, yh_recv.at[j, h], dp=across)

    def y_last(other=False):
        q = sided(quarter - 1, True)
        return remote(w_ref.at[1, q], wall.at[me_dp, 1, q], w_send, yh_recv.at[step_z, 0], dp=across)

    def side_copy(j, other=False):
        q = sided(j, other)
        ref = wall.at[across, 0, q] if j == quarter - 1 else w_of(across, q)
        return remote(ref, ref, w_send, wx_recv.at[j], sp=side)

    def near_copy(j, h, other=False):
        q = neighboured(j, other)
        return remote(wall.at[across, h, q], wall.at[across, h, q], w_send, wz_recv.at[j, h],
                      sp=other_z * 2 + x)

    def forward(q):
        return remote(w_of(across, q), w_of(across, q), w_send, w_recv.at[q], dp=partner)

    def p_copy(q):
        return remote(w_ref.at[:, q], w_of(me_dp, q), w_send, w_recv.at[q], dp=partner)

    def w_own(q):
        return pltpu.make_async_copy(w_ref.at[:, q], w_of(me_dp, q), w_recv.at[q])

    direct = pairs - 3
    ahead = min(3, pairs)

    def lead(makers):
        for p in range(ahead):
            for make in makers:
                z_own(*make, p).start()

    def gates_out():
        g_copy.start()
        g_own.start()

    @pl.when(z == 0)
    def _():
        gates_out()
        lead(up)
        for p in range(pairs):
            for a in (1, 2):
                x_copy(a, p).start()
        for p in range(pairs):
            x_copy(0, p).start()

    @pl.when(z == 1)
    def _():
        gates_out()
        for p in range(pairs):
            for a in (1, 2, 0):
                x_copy(a, p).start()

    @pl.when(z == 2)
    def _():
        for p in range(ahead):
            x_copy(0, p).start()
            if p == 0:
                lead(down_two)
            if p + direct < pairs:
                x_copy(0, p + direct).start()
        gates_out()
        for i in range(pairs):
            for a in (1, 2):
                x_copy(a, (i + direct) % pairs).start()
            if i + ahead < direct:
                x_copy(0, i + ahead).start()

    @pl.when(z == 3)
    def _():
        for p in range(direct):
            x_copy(0, p).start()
            if p + direct < pairs:
                x_copy(0, p + direct).start()
            if p == 0:
                for i in range(ahead):
                    z_own(0, 3, 1, i).start()
                    z_own(0, 2, 2, (i + direct) % pairs).start()
        gates_out()
        for p in range(pairs):
            for a in (1, 2):
                x_copy(a, p).start()

    for j in range(step_z):
        for h in range(2):
            y_half(j, h).start()
    for u in range(units):
        y_copy(u).start()
    y_last().start()
    for p in range(pairs):
        for a in range(3):
            x_own(a, p).start()

    def pass_on(u):
        y_copy(u).wait_recv()
        if u < quarter:
            side_copy(u).start()
        forward(y_pair(u)).start()

    def pass_loan(j):
        side_copy(j, True).wait_recv()
        if j == quarter - 1:
            y_last().wait_recv()
        forward(sided(j, True)).start()

    def near_here(h):
        for j in range(step_z):
            y_half(j, h).wait_recv()
            if h == 1:
                forward(neighboured(j, False)).start()

    def near_lend(h):
        for j in range(step_z):
            near_copy(j, h).start()

    def near_loan():
        for j in range(step_z):
            for h in range(2):
                near_copy(j, h, True).wait_recv()
            forward(neighboured(j, True)).start()

    def share_weights(p):
        p_copy(p).start()
        w_own(p).start()

    def part_copies(k, slot, p, target):
        return (
            remote(part_o.at[k, p], got_o.at[p, slot], po_send, po_recv.at[p], sp=target * 2 + x),
            remote(part_l.at[k, p], got_l.at[p, slot], pl_send, pl_recv.at[p], sp=target * 2 + x),
        )

    def o_copy(p):
        return remote(ob.at[p, rows_of(1 - x), :], att.at[p, :, half_of(x)], o_send, o_recv.at[p], sp=side)

    def gates_of(block, p):
        return jnp.concatenate([gb[2 * block, p], gb[2 * block + 1, p]], axis=1)

    def finish(p, value):
        ob[p] = value.astype(jnp.bfloat16)
        o_copy(p).start()
        att[p, :, half_of(x)] = ob[p, rows_of(x), :]

    final = pairs - 1

    def tail_copies(k, slot, target, row, o_sem, l_sem):
        return (
            remote(part_o.at[k, final, rows_of(row), :], tail_o.at[slot, x], o_sem, t_recv.at[slot, 0],
                   sp=target * 2 + row),
            remote(part_l.at[k, final, :, rows_of(row)], tail_l.at[slot, x], l_sem, t_recv.at[slot, 1],
                   sp=target * 2 + row),
        )

    def send_part(p, k, slot, target):
        @pl.when(p < final)
        def _():
            for copy in part_copies(k, slot, p, target):
                copy.start()

        @pl.when(p == final)
        def _():
            for row in (1 - x, x):
                for copy in tail_copies(k, slot, target, row, po_send, pl_send):
                    copy.start()

    def hold(p, value, lse):
        @pl.when(p < final)
        def _():
            held_o[p], held_l[p] = value, lse

        @pl.when(p == final)
        def _():
            store_part(final, 0, value, lse)
            for copy in tail_copies(0, 2, z, 1 - x, o_send, g_send.at[1]):
                copy.start()
            tail_o[2, pl.ds(x, 1)] = part_o[0, final, rows_of(x), :][None]
            tail_l[2, pl.ds(x, 1)] = part_l[0, final, :, rows_of(x)][None]

    def join_tail(slots):
        landed(tail_o.at[2, 1 - x], t_recv.at[2, 0])
        landed(tail_l.at[2, 1 - x], t_recv.at[2, 1])
        for slot in slots:
            landed(tail_o.at[slot], t_recv.at[slot, 0])
            landed(tail_l.at[slot], t_recv.at[slot, 1])
        for h in range(2):
            outs, sums = [], []
            for slot in (2,) + slots:
                outs.append(tail_o[slot, h].astype(jnp.float32))
                lse = tail_l[slot, h]
                sums.append(jnp.transpose(jnp.concatenate(
                    [jnp.broadcast_to(lse[j:j + 1], (HEAD_DIM, L)) for j in range(2)], axis=0)))
            peak = functools.reduce(jnp.maximum, sums)
            scale = [jnp.exp2(s - peak) for s in sums]
            value = sum(o * s for o, s in zip(outs, scale)) / sum(scale)
            att[final, :, h * LANES:(h + 1) * LANES] = value.astype(jnp.bfloat16)

    def share(p, k, slot, target, value, lse):
        store_part(p, k, value, lse)
        send_part(p, k, slot, target)

    def store_part(p, k, value, lse):
        part_o[k, p] = value.astype(jnp.bfloat16)
        turned = jnp.transpose(lse)
        part_l[k, p] = jnp.concatenate([turned[0:1], turned[HEAD_DIM:HEAD_DIM + 1]], axis=0)

    def merged(p, o_ref, l_ref, slots):
        outs, sums = [o_ref[p]], [l_ref[p]]
        for slot in slots:
            outs.append(got_o[p, slot].astype(jnp.float32))
            lse = got_l[p, slot]
            sums.append(jnp.transpose(jnp.concatenate(
                [jnp.broadcast_to(lse[h:h + 1], (HEAD_DIM, 2 * L)) for h in range(2)], axis=0)))
        peak = functools.reduce(jnp.maximum, sums)
        scale = [jnp.exp2(s - peak) for s in sums]
        total = sum(scale)
        return sum(o * s for o, s in zip(outs, scale)) / total, peak + jnp.log2(total)

    def parts_here(p, slots):
        landed(got_o.at[p] if len(slots) == 2 else got_o.at[p, slots[0]], po_recv.at[p])
        landed(got_l.at[p] if len(slots) == 2 else got_l.at[p, slots[0]], pl_recv.at[p])

    def join(p, slots):
        parts_here(p, slots)
        finish(p, merged(p, held_o, held_l, slots)[0])

    def join_two(p):
        @pl.when(p < direct)
        def _():
            parts_here(p, (0, 1))
            share(p, 1, 1, 3, *merged(p, near_o, near_l, (1,)))
            finish(p, merged(p, held_o, held_l, (0,))[0])

        @pl.when((p >= direct) & (p < final))
        def _():
            join(p, (0,))

        @pl.when(p == final)
        def _():
            join_tail((0,))

    def join_three(p):
        @pl.when(p < direct)
        def _():
            join(p, (1,))

        @pl.when((p >= direct) & (p < final))
        def _():
            join(p, (0, 1))

        @pl.when(p == final)
        def _():
            join_tail((0, 1))

    def each(body, begin=0, end=None):
        def step(p, carry):
            body(p)
            return carry
        lax.fori_loop(begin, pairs if end is None else end, step, 0)

    def gates_here():
        g_own.wait()
        g_copy.wait_recv()

    def gates_up(target):
        return remote(gb.at[pl.ds(0, 2)], gb.at[pl.ds(0, 2)], g_send.at[1], g_recv.at[2], sp=target * 2 + x)

    def passing(p, table):
        for at, calls in table.items():
            @pl.when(p == at)
            def _(calls=calls):
                for call in calls:
                    call()

    def on(u):
        return lambda: pass_on(u)

    def near_all():
        near_here(0)
        near_here(1)

    def near_lend_all():
        near_lend(0)
        near_lend(1)

    def push(p, makers):
        for make in makers:
            z_side(*make, p).start()
        @pl.when(p + ahead < pairs)
        def _():
            for make in makers:
                z_own(*make, p + ahead).start()

    early = [q for q in range(pairs // 2) if q != 1]
    late = [q for q in range(pairs) if q not in early]

    def products(which):
        for q in which:
            landed(wall.at[pl.ds(0, 3), :, q], w_recv.at[q])
            if q < final:
                o_copy(q).wait_recv()
            else:
                @pl.when(z < 2)
                def _():
                    o_copy(q).wait_recv()
            lhs = att[q]
            for r in range(ndp):
                columns = slice(r * w_cols, (r + 1) * w_cols)
                part = jnp.dot(lhs, wall[r, :, q].reshape(2 * LANES, w_cols), preferred_element_type=jnp.float32)
                if q != early[0]:
                    part = acc[:, columns] + part
                if q < final:
                    acc[:, columns] = part
                else:
                    o_ref[:, columns] = part.astype(o_ref.dtype)

    def first_products():
        products(early)

    @pl.when(z == 0)
    def _():
        def pushes(p):
            keys_here(p)
            push(p, up)
        gates_here()
        gates_up(1).start()
        each(pushes)
        def work(p):
            queries_here(p)
            finish(p, attend_rows([(qx[p], True)], [(kvx[p, 0], kvx[p, 1], gates_of(0, p))])[0][0])
            share_weights(p)
            passing(p, {0: [near_all], 3: [on(0)], 7: [on(1)]})
        each(work)
        near_lend_all()
        near_loan()
        pass_on(2)

    @pl.when(z == 1)
    def _():
        gates_here()
        gates_up(0).wait_recv()
        def work(p):
            keys_here(p)
            landed(zin.at[p], z_recv.at[p])
            lower = (zin[p, 0], zin[p, 1], gates_of(0, p))
            own = (kvx[p, 0], kvx[p, 1], gates_of(1, p))
            queries_here(p)
            three, two, one = attend_rows([(zin[p, 3], False), (zin[p, 2], False), (qx[p], True)], [lower, own])
            share(p, 0, 0, 2, *two)
            store_part(p, 1, *three)
            @pl.when(p < direct)
            def _():
                send_part(p, 1, 1, 2)

            @pl.when(p >= direct)
            def _():
                send_part(p, 1, 0, 3)
            finish(p, one[0])
            share_weights(p)
            passing(p, {0: [near_all, near_lend_all], 2: [on(0)], 4: [on(1)], 7: [on(2)]})
        each(work)

    @pl.when(z == 2)
    def _():
        for p in range(ahead):
            queries_here(p)
            push(p, down_two)
            if p + direct < pairs:
                queries_here(p + direct)
        near_here(0)
        near_lend(0)
        gates_here()
        lag = pairs - direct
        def work(i):
            p = lax.rem(i + direct, pairs)
            keys_here(p)
            own = (kvx[p, 0], kvx[p, 1], gates_of(2, p))
            landed(zin.at[p, 2], z_recv.at[p])
            (near_o[p], near_l[p]), mine = attend_rows([(zin[p, 2], False), (qx[p], True)], [own])
            hold(p, *mine)
            @pl.when(p >= direct)
            def _():
                share(p, 1, 1, 3, near_o[p], near_l[p])
            @pl.when(i + ahead < pairs)
            def _():
                @pl.when(i + ahead < direct)
                def _():
                    queries_here(i + ahead)
                push(i + ahead, down_two)
            passing(i, {0: [lambda: near_here(1), lambda: near_lend(1)], 3: [on(0)], 5: [on(1)]})
            @pl.when(i >= lag)
            def _():
                join_two(i - lag)
            share_weights(p)
            passing(i, {pairs - 1: [on(2)]})
        each(work)
        def last(p):
            join_two(p)
            passing(p, {direct: [lambda: pass_loan(0), near_loan], pairs - 2: [first_products, on(3), lambda: pass_loan(1)]})
        each(last, direct)

    @pl.when(z == 3)
    def _():
        for i in range(pairs):
            if i < direct:
                queries_here(i)
            if i + direct < pairs:
                queries_here(i + direct)
            near = (i + direct) % pairs
            z_side(0, 3, 1, i).start()
            z_side(0, 2, 2, near).start()
            if i + ahead < pairs:
                z_own(0, 3, 1, i + ahead).start()
                z_own(0, 2, 2, (near + ahead) % pairs).start()
        gates_here()
        def work(p):
            keys_here(p)
            hold(p, *attend_rows([(qx[p], True)], [(kvx[p, 0], kvx[p, 1], gates_of(3, p))])[0])
            share_weights(p)
            passing(p, {0: [near_all, near_lend_all], 4: [on(0)], 7: [near_loan, on(1)]})
        each(work)
        def last(p):
            join_three(p)
            passing(p, {3: [on(2)], 4: [lambda: pass_loan(0)], 6: [on(3), lambda: pass_loan(1)], 7: [first_products]})
        each(last)

    @pl.when(z == 0)
    def _():
        pass_loan(0)
        first_products()
        pass_on(3)
        pass_loan(1)

    @pl.when(z == 1)
    def _():
        pass_loan(0)
        near_loan()
        first_products()
        pass_on(3)
        pass_loan(1)

    products(late)

    g_copy.wait_send()

    @pl.when(z == 0)
    def _():
        left(wall.at[0, 0], z_send)
        gates_up(1).wait_send()

    @pl.when(z == 1)
    def _():
        left(part_o, po_send)
        left(part_l, pl_send)

    @pl.when(z == 2)
    def _():
        left(wall.at[0, 0, pl.ds(0, pairs // 2)], z_send)
        left(part_o.at[1], po_send)
        left(part_l.at[1], pl_send)

    @pl.when(z == 3)
    def _():
        left(wall.at[0, 0], z_send)

    @pl.when(z >= 2)
    def _():
        left(part_l.at[0, final, :, rows_of(1 - x)], g_send.at[1])

    left(ob.at[:, pl.ds(0, L), :], o_send)
    left(wall.at[0, 0, pl.ds(0, 3 * pairs // 4)], x_send)
    left(wall.at[pl.ds(0, 3)], w_send)


def fused(n, ndp, queries, keys, values, gate_totals, w_out):
    L, model = queries.shape[1], queries.shape[2]
    heads = gate_totals.shape[2] // 2
    pairs = heads * HEAD_DIM // LANES
    gates = jnp.transpose(gate_totals[0]).reshape(2, pairs, 2, L)
    w_cols = w_out.shape[1]
    weights = w_out.reshape(2, pairs, LANES, w_cols)
    bf16, f32 = jnp.bfloat16, jnp.float32
    dma = pltpu.SemaphoreType.DMA
    block = (pairs, 2 * L, LANES)
    quarter = pairs // 4
    units, step_z = 2 * quarter, quarter // 2
    out = pl.pallas_call(
        functools.partial(kernel, n, ndp),
        out_shape=jax.ShapeDtypeStruct((L, w_cols * ndp), bf16),
        in_specs=[pl.BlockSpec(memory_space=pltpu.HBM)] * 5,
        out_specs=pl.BlockSpec(memory_space=pltpu.VMEM),
        scratch_shapes=[
            pltpu.VMEM(block, bf16),
            pltpu.VMEM((pairs, 2) + block[1:], bf16),
            pltpu.VMEM((pairs, 4) + block[1:], bf16),
            pltpu.VMEM((n, pairs, 2, L), f32),
            pltpu.VMEM(block, bf16),
            *[pltpu.VMEM(block, f32)] * 4,
            pltpu.VMEM((2,) + block, bf16),
            pltpu.VMEM((2, pairs, 2, 2 * L), f32),
            pltpu.VMEM((pairs, 2) + block[1:], bf16),
            pltpu.VMEM((pairs, 2, 2, 2 * L), f32),
            pltpu.VMEM((3, 2, L, LANES), bf16),
            pltpu.VMEM((3, 2, 2, L), f32),
            pltpu.VMEM((pairs, L, 2 * LANES), bf16),
            pltpu.VMEM((ndp, 2, pairs, LANES, w_cols), bf16),
            pltpu.VMEM((L, ndp * w_cols), f32),
            dma((pairs,)), dma((pairs,)), dma, dma((2,)), dma((3,)), dma, dma((pairs,)),
            dma, dma((pairs,)), dma, dma((pairs,)),
            dma, dma((pairs,)), dma((3, 2)), dma((units,)), dma((step_z + 1, 2)), dma((quarter,)), dma((step_z, 2)),
            dma((pairs,)), dma,
        ],
        compiler_params=pltpu.CompilerParams(
            collective_id=0, has_side_effects=True, vmem_limit_bytes=48 * 2**20),
        name="fused_attention",
    )(*[pltpu.with_memory_space_constraint(t, pltpu.HBM) for t in (queries[0], keys[0], values[0], gates, weights)])
    return out[None]


def solution(mesh):
    n, ndp = mesh.shape["sp"], mesh.shape["dp"]

    def local(queries, keys, values, gate_totals, w_out):
        fits = n == 8 and ndp == 4 and queries.shape[1] % LANES == 0 and queries.shape[2] == 2 * n * LANES
        if fits:
            return fused(n, ndp, queries, keys, values, gate_totals, w_out)
        return general(queries, keys, values, gate_totals, w_out)

    placed = (P("dp", "sp", None),) * 4 + (P(None, "dp"),)
    return jax.shard_map(
        local, mesh=mesh, in_specs=placed, out_specs=P("dp", "sp", None), check_vma=False)
```

```python
import functools

import jax
import jax.numpy as jnp
from jax import lax
from jax.experimental import pallas as pl
from jax.experimental.pallas import tpu as pltpu
from jax.sharding import PartitionSpec as P

HEAD_DIM = 64
LANES = 128
LOG2E = 1.4426950408889634
MESH = pl.DeviceIdType.MESH


def attend(queries, key_rows, value_rows, totals):
    length = queries.shape[0]
    block_rows = min(length, 512)
    pieces = []
    for begin_row in range(0, length, block_rows):
        end_row = begin_row + block_rows
        scaled = queries[begin_row:end_row] * jnp.bfloat16(HEAD_DIM ** (-0.5))
        scores = jnp.einsum(
            "qhd,khd->hqk", scaled, key_rows[:end_row], preferred_element_type=jnp.float32
        )
        causal = jnp.arange(end_row)[None, :] <= (begin_row + jnp.arange(block_rows))[:, None]
        scores = jnp.where(
            causal[None],
            scores
            + jnp.transpose(totals[begin_row:end_row])[:, :, None]
            - jnp.transpose(totals[:end_row])[:, None, :],
            -jnp.inf,
        )
        biggest = jnp.max(scores, axis=-1, keepdims=True)
        expo = jnp.exp(scores - biggest)
        summed = jnp.sum(expo, axis=-1)
        weights = expo.astype(jnp.bfloat16)
        output = jnp.einsum(
            "hqk,khd->qhd", weights, value_rows[:end_row], preferred_element_type=jnp.float32
        )
        output = output / jnp.transpose(summed)[:, :, None]
        pieces.append(output.astype(jnp.bfloat16))
    return jnp.concatenate(pieces, axis=0).reshape(length, -1)


def general(queries, keys, values, gate_totals, w_out):
    moved = [
        lax.all_to_all(x, "sp", split_axis=2, concat_axis=1, tiled=True)
        for x in (queries, keys, values, gate_totals)
    ]
    length = moved[0].shape[1]
    heads = [x[0].reshape(length, -1, HEAD_DIM) for x in moved[:3]]
    attended = attend(heads[0], heads[1], heads[2], moved[3][0])[None]
    rows = lax.all_to_all(attended, "sp", split_axis=1, concat_axis=2, tiled=True)
    mixed = jnp.dot(
        rows[0],
        lax.all_gather(w_out, "dp", axis=1, tiled=True),
        preferred_element_type=jnp.float32,
    )
    return mixed.astype(jnp.bfloat16)[None]


def attend_rows(tasks, parts):
    def of_head(h, array, other):
        lane = lax.broadcasted_iota(jnp.int32, array.shape, 1)
        return jnp.where((lane < HEAD_DIM) if h == 0 else (lane >= HEAD_DIM), array, jnp.full_like(array, other))

    chains = [(i, h) for i in range(len(tasks)) for h in range(2)]
    scaled = [queries * jnp.bfloat16(HEAD_DIM ** -0.5) for queries, _ in tasks]
    head_keys = [[of_head(h, part[0], 0) for part in parts] for h in range(2)]
    head_values = [[of_head(h, part[1], 1) for part in parts] for h in range(2)]
    gates = [part[2] * LOG2E for part in parts]
    scores, peaks, weights, sums = {}, {}, {}, {}
    for i, h in chains:
        scores[i, h] = [
            lax.dot_general(scaled[i], keys, (((1,), (1,)), ((), ())), preferred_element_type=jnp.float32)
            for keys in head_keys[h]]
    for i, h in chains:
        rows = [score * LOG2E - gate[h:h + 1, :] for score, gate in zip(scores[i, h], gates)]
        if tasks[i][1]:
            shape = rows[-1].shape
            causal = lax.broadcasted_iota(jnp.int32, shape, 1) <= lax.broadcasted_iota(jnp.int32, shape, 0)
            rows[-1] = jnp.where(causal, rows[-1], -jnp.inf)
        scores[i, h] = rows
        peaks[i, h] = functools.reduce(jnp.maximum, [jnp.max(x, axis=1, keepdims=True) for x in rows])
    for i, h in chains:
        weights[i, h] = [jnp.exp2(x - peaks[i, h]).astype(jnp.bfloat16) for x in scores[i, h]]
    for i, h in chains:
        sums[i, h] = sum(
            jnp.dot(x, values, preferred_element_type=jnp.float32)
            for x, values in zip(weights[i, h], head_values[h]))
    results = []
    for i in range(len(tasks)):
        first = lax.broadcasted_iota(jnp.int32, sums[i, 0].shape, 1) < HEAD_DIM
        out = jnp.where(first, sums[i, 0], sums[i, 1])
        total = pltpu.roll(jnp.where(first, sums[i, 1], sums[i, 0]), HEAD_DIM, 1)
        results.append((out / total, jnp.where(first, peaks[i, 0], peaks[i, 1]) + jnp.log2(total)))
    return results


def kernel(n, ndp, q_ref, k_ref, v_ref, g_ref, w_ref, o_ref,
           qx, kvx, zin, gb, ob, held_o, held_l, near_o, near_l, part_o, part_l, got_o, got_l, tail_o, tail_l, att, wall, acc,
           q_recv, kv_recv, x_send, g_send, g_recv, z_send, z_recv, po_send, po_recv, pl_send, pl_recv,
           o_send, o_recv, t_recv, y_recv, yh_recv, wx_recv, wz_recv, w_recv, w_send):
    me = lax.axis_index("sp")
    x = lax.rem(me, 2)
    z = lax.div(me, 2)
    side = me + 1 - 2 * x
    me_dp = lax.axis_index("dp")
    core = lax.rem(me_dp, 2)
    row_y = lax.div(me_dp, 2)
    across = (1 - row_y) * 2 + core
    partner = row_y * 2 + 1 - core
    L = q_ref.shape[0]
    pairs = qx.shape[0]
    W = pairs * LANES
    w_cols = w_ref.shape[3]
    quarter = pairs // 4
    units = quarter * 2
    step_z = quarter // 2
    odd = lax.rem(z, 2)
    other_z = z + 1 - 2 * odd

    barrier = pltpu.get_barrier_semaphore()
    meets = {0: (1,), 1: (0, 2, 3), 2: (1, 3), 3: (1, 2)}
    for here, others in meets.items():
        @pl.when(z == here)
        def _(others=others):
            for other in others:
                pl.semaphore_signal(barrier, inc=1, device_id={"sp": other * 2 + x}, device_id_type=MESH)
    pl.semaphore_signal(barrier, inc=1, device_id={"sp": side}, device_id_type=MESH)
    for other in (partner, across):
        pl.semaphore_signal(barrier, inc=1, device_id={"dp": other}, device_id_type=MESH)
    for here, others in meets.items():
        @pl.when(z == here)
        def _(others=others):
            pl.semaphore_wait(barrier, len(others) + 3)

    def remote(src, dst, send, recv, **device):
        return pltpu.make_async_remote_copy(
            src_ref=src, dst_ref=dst, send_sem=send, recv_sem=recv, device_id=device, device_id_type=MESH)

    def rows_of(which):
        return pl.ds(pl.multiple_of(which * L, L), L)

    def lanes_of(which, p):
        return pl.ds(pl.multiple_of(which * W + p * LANES, LANES), LANES)

    def half_of(which):
        return pl.ds(pl.multiple_of(which * LANES, LANES), LANES)

    def landing(a, p):
        return qx.at[p] if a == 0 else kvx.at[p, a - 1]

    refs = (q_ref, k_ref, v_ref)

    def x_sem(a, p):
        return q_recv.at[p] if a == 0 else kv_recv.at[p]

    def x_copy(a, p):
        return remote(refs[a].at[:, lanes_of(1 - x, p)], landing(a, p).at[rows_of(x), :], x_send, x_sem(a, p), sp=side)

    def x_own(a, p):
        return pltpu.make_async_copy(refs[a].at[:, lanes_of(x, p)], landing(a, p).at[rows_of(x), :], x_sem(a, p))

    def landed(ref, sem):
        remote(ref, ref, x_send, sem, sp=side).wait_recv()

    def left(ref, sem):
        remote(ref, ref, sem, w_recv.at[0], sp=side).wait_send()

    def queries_here(p):
        landed(qx.at[p], q_recv.at[p])

    def keys_here(p):
        landed(kvx.at[p], kv_recv.at[p])

    g_copy = remote(g_ref.at[1 - x], gb.at[me], g_send.at[0], g_recv.at[0], sp=side)
    g_own = pltpu.make_async_copy(g_ref.at[x], gb.at[me], g_recv.at[1])

    def z_own(a, slot, target, p):
        return remote(refs[a].at[:, lanes_of(x, p)], zin.at[p, slot, rows_of(x), :],
                      z_send, z_recv.at[p], sp=target * 2 + x)

    def z_side(a, slot, target, p):
        return remote(landing(a, p).at[rows_of(1 - x), :], zin.at[p, slot, rows_of(1 - x), :],
                      z_send, z_recv.at[p], sp=target * 2 + x)

    up = ((1, 0, 1), (2, 1, 1))
    down_two = ((0, 2, 1),)

    def sided(j, other):
        which = 1 - x if other else x
        return pairs // 2 + j + quarter * which

    def neighboured(j, other):
        which = 1 - odd if other else odd
        return quarter + j + step_z * which

    def w_of(r, q):
        return wall.at[r, :, q]

    def y_pair(u):
        return sided(u, False) if u < quarter else u - quarter

    def y_copy(u):
        return remote(w_ref.at[:, y_pair(u)], w_of(me_dp, y_pair(u)), w_send, y_recv.at[u], dp=across)

    def y_half(j, h):
        q = neighboured(j, False)
        return remote(w_ref.at[h, q], wall.at[me_dp, h, q], w_send, yh_recv.at[j, h], dp=across)

    def y_last(other=False):
        q = sided(quarter - 1, True)
        return remote(w_ref.at[1, q], wall.at[me_dp, 1, q], w_send, yh_recv.at[step_z, 0], dp=across)

    def side_copy(j, other=False):
        q = sided(j, other)
        ref = wall.at[across, 0, q] if j == quarter - 1 else w_of(across, q)
        return remote(ref, ref, w_send, wx_recv.at[j], sp=side)

    def near_copy(j, h, other=False):
        q = neighboured(j, other)
        return remote(wall.at[across, h, q], wall.at[across, h, q], w_send, wz_recv.at[j, h],
                      sp=other_z * 2 + x)

    def forward(q):
        return remote(w_of(across, q), w_of(across, q), w_send, w_recv.at[q], dp=partner)

    def p_copy(q):
        return remote(w_ref.at[:, q], w_of(me_dp, q), w_send, w_recv.at[q], dp=partner)

    def w_own(q):
        return pltpu.make_async_copy(w_ref.at[:, q], w_of(me_dp, q), w_recv.at[q])

    direct = pairs - 3
    ahead = min(3, pairs)

    def lead(makers):
        for p in range(ahead - (len(makers) > 1)):
            for make in makers:
                z_own(*make, p).start()

    def gates_out():
        g_copy.start()
        g_own.start()

    @pl.when(z == 0)
    def _():
        gates_out()
        lead(up)
        for p in range(pairs):
            for a in (1, 2):
                x_copy(a, p).start()
        for p in range(pairs):
            x_copy(0, p).start()

    @pl.when(z == 1)
    def _():
        gates_out()
        for p in range(pairs):
            for a in (1, 2, 0):
                x_copy(a, p).start()

    @pl.when(z == 2)
    def _():
        for p in range(ahead):
            x_copy(0, p).start()
            if p == 0:
                lead(down_two)
            if p + direct < pairs:
                x_copy(0, p + direct).start()
        gates_out()
        for i in range(pairs):
            for a in (1, 2):
                x_copy(a, (i + direct) % pairs).start()
            if i + ahead < direct:
                x_copy(0, i + ahead).start()

    @pl.when(z == 3)
    def _():
        for p in range(direct):
            x_copy(0, p).start()
            if p + direct < pairs:
                x_copy(0, p + direct).start()
            if p == 0:
                for i in range(ahead):
                    z_own(0, 3, 1, i).start()
                    z_own(0, 2, 2, (i + direct) % pairs).start()
        gates_out()
        for p in range(pairs):
            for a in (1, 2):
                x_copy(a, p).start()

    for j in range(step_z):
        for h in range(2):
            y_half(j, h).start()
    for u in range(units):
        y_copy(u).start()
    y_last().start()
    for p in range(pairs):
        for a in range(3):
            x_own(a, p).start()

    def pass_on(u):
        y_copy(u).wait_recv()
        if u < quarter:
            side_copy(u).start()
        forward(y_pair(u)).start()

    def pass_loan(j):
        side_copy(j, True).wait_recv()
        if j == quarter - 1:
            y_last().wait_recv()
        forward(sided(j, True)).start()

    def near_here(h):
        for j in range(step_z):
            y_half(j, h).wait_recv()
            if h == 1:
                forward(neighboured(j, False)).start()

    def near_lend(h):
        for j in range(step_z):
            near_copy(j, h).start()

    def near_loan():
        for j in range(step_z):
            for h in range(2):
                near_copy(j, h, True).wait_recv()
            forward(neighboured(j, True)).start()

    def share_weights(p):
        p_copy(p).start()
        w_own(p).start()

    def part_copies(k, slot, p, target):
        return (
            remote(part_o.at[k, p], got_o.at[p, slot], po_send, po_recv.at[p], sp=target * 2 + x),
            remote(part_l.at[k, p], got_l.at[p, slot], pl_send, pl_recv.at[p], sp=target * 2 + x),
        )

    def o_copy(p):
        return remote(ob.at[p, rows_of(1 - x), :], att.at[p, :, half_of(x)], o_send, o_recv.at[p], sp=side)

    def gates_of(block, p):
        return jnp.concatenate([gb[2 * block, p], gb[2 * block + 1, p]], axis=1)

    def finish(p, value):
        ob[p] = value.astype(jnp.bfloat16)
        o_copy(p).start()
        att[p, :, half_of(x)] = ob[p, rows_of(x), :]

    final = pairs - 1

    def tail_copies(k, slot, target, row, o_sem, l_sem):
        return (
            remote(part_o.at[k, final, rows_of(row), :], tail_o.at[slot, x], o_sem, t_recv.at[slot, 0],
                   sp=target * 2 + row),
            remote(part_l.at[k, final, :, rows_of(row)], tail_l.at[slot, x], l_sem, t_recv.at[slot, 1],
                   sp=target * 2 + row),
        )

    def send_part(p, k, slot, target):
        @pl.when(p < final)
        def _():
            for copy in part_copies(k, slot, p, target):
                copy.start()

        @pl.when(p == final)
        def _():
            for row in (1 - x, x):
                for copy in tail_copies(k, slot, target, row, po_send, pl_send):
                    copy.start()

    def hold(p, value, lse):
        @pl.when(p < final)
        def _():
            held_o[p], held_l[p] = value, lse

        @pl.when(p == final)
        def _():
            store_part(final, 0, value, lse)
            for copy in tail_copies(0, 2, z, 1 - x, o_send, g_send.at[1]):
                copy.start()
            tail_o[2, pl.ds(x, 1)] = part_o[0, final, rows_of(x), :][None]
            tail_l[2, pl.ds(x, 1)] = part_l[0, final, :, rows_of(x)][None]

    def join_tail(slots):
        landed(tail_o.at[2, 1 - x], t_recv.at[2, 0])
        landed(tail_l.at[2, 1 - x], t_recv.at[2, 1])
        for slot in slots:
            landed(tail_o.at[slot], t_recv.at[slot, 0])
            landed(tail_l.at[slot], t_recv.at[slot, 1])
        for h in range(2):
            outs, sums = [], []
            for slot in (2,) + slots:
                outs.append(tail_o[slot, h].astype(jnp.float32))
                lse = tail_l[slot, h]
                sums.append(jnp.transpose(jnp.concatenate(
                    [jnp.broadcast_to(lse[j:j + 1], (HEAD_DIM, L)) for j in range(2)], axis=0)))
            peak = functools.reduce(jnp.maximum, sums)
            scale = [jnp.exp2(s - peak) for s in sums]
            value = sum(o * s for o, s in zip(outs, scale)) / sum(scale)
            att[final, :, h * LANES:(h + 1) * LANES] = value.astype(jnp.bfloat16)

    def share(p, k, slot, target, value, lse):
        store_part(p, k, value, lse)
        send_part(p, k, slot, target)

    def store_part(p, k, value, lse):
        part_o[k, p] = value.astype(jnp.bfloat16)
        turned = jnp.transpose(lse)
        part_l[k, p] = jnp.concatenate([turned[0:1], turned[HEAD_DIM:HEAD_DIM + 1]], axis=0)

    def merged(p, o_ref, l_ref, slots):
        outs, sums = [o_ref[p]], [l_ref[p]]
        for slot in slots:
            outs.append(got_o[p, slot].astype(jnp.float32))
            lse = got_l[p, slot]
            sums.append(jnp.transpose(jnp.concatenate(
                [jnp.broadcast_to(lse[h:h + 1], (HEAD_DIM, 2 * L)) for h in range(2)], axis=0)))
        peak = functools.reduce(jnp.maximum, sums)
        scale = [jnp.exp2(s - peak) for s in sums]
        total = sum(scale)
        return sum(o * s for o, s in zip(outs, scale)) / total, peak + jnp.log2(total)

    def parts_here(p, slots):
        landed(got_o.at[p] if len(slots) == 2 else got_o.at[p, slots[0]], po_recv.at[p])
        landed(got_l.at[p] if len(slots) == 2 else got_l.at[p, slots[0]], pl_recv.at[p])

    def join(p, slots):
        parts_here(p, slots)
        finish(p, merged(p, held_o, held_l, slots)[0])

    def join_two(p):
        @pl.when(p < direct)
        def _():
            parts_here(p, (0, 1))
            share(p, 1, 1, 3, *merged(p, near_o, near_l, (1,)))
            finish(p, merged(p, held_o, held_l, (0,))[0])

        @pl.when((p >= direct) & (p < final))
        def _():
            join(p, (0,))

        @pl.when(p == final)
        def _():
            join_tail((0,))

    def join_three(p):
        @pl.when(p < direct)
        def _():
            join(p, (1,))

        @pl.when((p >= direct) & (p < final))
        def _():
            join(p, (0, 1))

        @pl.when(p == final)
        def _():
            join_tail((0, 1))

    def each(body, begin=0, end=None):
        def step(p, carry):
            body(p)
            return carry
        lax.fori_loop(begin, pairs if end is None else end, step, 0)

    def gates_here():
        g_own.wait()
        g_copy.wait_recv()

    def gates_up(target):
        return remote(gb.at[pl.ds(0, 2)], gb.at[pl.ds(0, 2)], g_send.at[1], g_recv.at[2], sp=target * 2 + x)

    def passing(p, table):
        for at, calls in table.items():
            @pl.when(p == at)
            def _(calls=calls):
                for call in calls:
                    call()

    def on(u):
        return lambda: pass_on(u)

    def near_all():
        near_here(0)
        near_here(1)

    def near_lend_all():
        near_lend(0)
        near_lend(1)

    def push(p, makers):
        reach = ahead - (len(makers) > 1)
        for make in makers:
            z_side(*make, p).start()
        @pl.when(p + reach < pairs)
        def _():
            for make in makers:
                z_own(*make, p + reach).start()

    early = [q for q in range(pairs // 2) if q != 1]
    late = [q for q in range(pairs - 2) if q not in early] + [pairs - 1, pairs - 2]

    def products(which):
        for q in which:
            landed(wall.at[pl.ds(0, 3), :, q], w_recv.at[q])
            if q < final:
                o_copy(q).wait_recv()
            else:
                @pl.when(z < 2)
                def _():
                    o_copy(q).wait_recv()
            lhs = att[q]
            for r in range(ndp):
                columns = slice(r * w_cols, (r + 1) * w_cols)
                part = jnp.dot(lhs, wall[r, :, q].reshape(2 * LANES, w_cols), preferred_element_type=jnp.float32)
                if q != early[0]:
                    part = acc[:, columns] + part
                if q != late[-1]:
                    acc[:, columns] = part
                else:
                    o_ref[:, columns] = part.astype(o_ref.dtype)

    def first_products():
        products(early)

    @pl.when(z == 0)
    def _():
        def pushes(p):
            keys_here(p)
            push(p, up)
        gates_here()
        gates_up(1).start()
        each(pushes)
        def work(p):
            queries_here(p)
            finish(p, attend_rows([(qx[p], True)], [(kvx[p, 0], kvx[p, 1], gates_of(0, p))])[0][0])
            share_weights(p)
            passing(p, {0: [near_all], 3: [on(0)], 7: [on(1)]})
        each(work)
        near_lend_all()
        near_loan()
        pass_on(2)

    @pl.when(z == 1)
    def _():
        gates_here()
        gates_up(0).wait_recv()
        def work(p):
            keys_here(p)
            landed(zin.at[p], z_recv.at[p])
            lower = (zin[p, 0], zin[p, 1], gates_of(0, p))
            own = (kvx[p, 0], kvx[p, 1], gates_of(1, p))
            queries_here(p)
            three, two, one = attend_rows([(zin[p, 3], False), (zin[p, 2], False), (qx[p], True)], [lower, own])
            share(p, 0, 0, 2, *two)
            store_part(p, 1, *three)
            @pl.when(p < direct)
            def _():
                send_part(p, 1, 1, 2)

            @pl.when(p >= direct)
            def _():
                send_part(p, 1, 0, 3)
            finish(p, one[0])
            share_weights(p)
            passing(p, {0: [near_all, near_lend_all], 2: [on(0)], 4: [on(1)], 7: [on(2)]})
        each(work)

    @pl.when(z == 2)
    def _():
        for p in range(ahead):
            queries_here(p)
            push(p, down_two)
            if p + direct < pairs:
                queries_here(p + direct)
        near_here(0)
        near_lend(0)
        gates_here()
        lag = pairs - direct
        def work(i):
            p = lax.rem(i + direct, pairs)
            keys_here(p)
            own = (kvx[p, 0], kvx[p, 1], gates_of(2, p))
            landed(zin.at[p, 2], z_recv.at[p])
            (near_o[p], near_l[p]), mine = attend_rows([(zin[p, 2], False), (qx[p], True)], [own])
            hold(p, *mine)
            @pl.when(p >= direct)
            def _():
                share(p, 1, 1, 3, near_o[p], near_l[p])
            @pl.when(i + ahead < pairs)
            def _():
                @pl.when(i + ahead < direct)
                def _():
                    queries_here(i + ahead)
                push(i + ahead, down_two)
            passing(i, {0: [lambda: near_here(1), lambda: near_lend(1)], 3: [on(0)], 5: [on(1)]})
            @pl.when(i >= lag)
            def _():
                join_two(i - lag)
            share_weights(p)
            passing(i, {pairs - 1: [on(2)]})
        each(work)
        def last(p):
            join_two(p)
            passing(p, {direct: [lambda: pass_loan(0), near_loan], pairs - 2: [first_products, on(3), lambda: pass_loan(1)]})
        each(last, direct)

    @pl.when(z == 3)
    def _():
        for i in range(pairs):
            if i < direct:
                queries_here(i)
            if i + direct < pairs:
                queries_here(i + direct)
            near = (i + direct) % pairs
            z_side(0, 3, 1, i).start()
            z_side(0, 2, 2, near).start()
            if i + ahead < pairs:
                z_own(0, 3, 1, i + ahead).start()
                z_own(0, 2, 2, (near + ahead) % pairs).start()
        gates_here()
        def work(p):
            keys_here(p)
            hold(p, *attend_rows([(qx[p], True)], [(kvx[p, 0], kvx[p, 1], gates_of(3, p))])[0])
            share_weights(p)
            passing(p, {0: [near_all, near_lend_all], 4: [on(0)], 7: [near_loan, on(1)]})
        each(work)
        def last(p):
            join_three(p)
            passing(p, {3: [on(2)], 4: [lambda: pass_loan(0)], 6: [on(3), lambda: pass_loan(1)], 7: [first_products]})
        each(last)

    @pl.when(z == 0)
    def _():
        pass_loan(0)
        first_products()
        pass_on(3)
        pass_loan(1)

    @pl.when(z == 1)
    def _():
        pass_loan(0)
        near_loan()
        first_products()
        pass_on(3)
        pass_loan(1)

    products(late)

    g_copy.wait_send()

    @pl.when(z == 0)
    def _():
        left(wall.at[0, 0], z_send)
        gates_up(1).wait_send()

    @pl.when(z == 1)
    def _():
        left(part_o, po_send)
        left(part_l, pl_send)

    @pl.when(z == 2)
    def _():
        left(wall.at[0, 0, pl.ds(0, pairs // 2)], z_send)
        left(part_o.at[1], po_send)
        left(part_l.at[1], pl_send)

    @pl.when(z == 3)
    def _():
        left(wall.at[0, 0], z_send)

    @pl.when(z >= 2)
    def _():
        left(part_l.at[0, final, :, rows_of(1 - x)], g_send.at[1])

    left(ob.at[:, pl.ds(0, L), :], o_send)
    left(wall.at[0, 0, pl.ds(0, 3 * pairs // 4)], x_send)
    left(wall.at[pl.ds(0, 3)], w_send)


def fused(n, ndp, queries, keys, values, gate_totals, w_out):
    L, model = queries.shape[1], queries.shape[2]
    heads = gate_totals.shape[2] // 2
    pairs = heads * HEAD_DIM // LANES
    gates = jnp.transpose(gate_totals[0]).reshape(2, pairs, 2, L)
    w_cols = w_out.shape[1]
    weights = w_out.reshape(2, pairs, LANES, w_cols)
    bf16, f32 = jnp.bfloat16, jnp.float32
    dma = pltpu.SemaphoreType.DMA
    block = (pairs, 2 * L, LANES)
    quarter = pairs // 4
    units, step_z = 2 * quarter, quarter // 2
    out = pl.pallas_call(
        functools.partial(kernel, n, ndp),
        out_shape=jax.ShapeDtypeStruct((L, w_cols * ndp), bf16),
        in_specs=[pl.BlockSpec(memory_space=pltpu.HBM)] * 5,
        out_specs=pl.BlockSpec(memory_space=pltpu.VMEM),
        scratch_shapes=[
            pltpu.VMEM(block, bf16),
            pltpu.VMEM((pairs, 2) + block[1:], bf16),
            pltpu.VMEM((pairs, 4) + block[1:], bf16),
            pltpu.VMEM((n, pairs, 2, L), f32),
            pltpu.VMEM(block, bf16),
            *[pltpu.VMEM(block, f32)] * 4,
            pltpu.VMEM((2,) + block, bf16),
            pltpu.VMEM((2, pairs, 2, 2 * L), f32),
            pltpu.VMEM((pairs, 2) + block[1:], bf16),
            pltpu.VMEM((pairs, 2, 2, 2 * L), f32),
            pltpu.VMEM((3, 2, L, LANES), bf16),
            pltpu.VMEM((3, 2, 2, L), f32),
            pltpu.VMEM((pairs, L, 2 * LANES), bf16),
            pltpu.VMEM((ndp, 2, pairs, LANES, w_cols), bf16),
            pltpu.VMEM((L, ndp * w_cols), f32),
            dma((pairs,)), dma((pairs,)), dma, dma((2,)), dma((3,)), dma, dma((pairs,)),
            dma, dma((pairs,)), dma, dma((pairs,)),
            dma, dma((pairs,)), dma((3, 2)), dma((units,)), dma((step_z + 1, 2)), dma((quarter,)), dma((step_z, 2)),
            dma((pairs,)), dma,
        ],
        compiler_params=pltpu.CompilerParams(
            collective_id=0, has_side_effects=True, vmem_limit_bytes=48 * 2**20),
        name="fused_attention",
    )(*[pltpu.with_memory_space_constraint(t, pltpu.HBM) for t in (queries[0], keys[0], values[0], gates, weights)])
    return out[None]


def solution(mesh):
    n, ndp = mesh.shape["sp"], mesh.shape["dp"]

    def local(queries, keys, values, gate_totals, w_out):
        fits = n == 8 and ndp == 4 and queries.shape[1] % LANES == 0 and queries.shape[2] == 2 * n * LANES
        if fits:
            return fused(n, ndp, queries, keys, values, gate_totals, w_out)
        return general(queries, keys, values, gate_totals, w_out)

    placed = (P("dp", "sp", None),) * 4 + (P(None, "dp"),)
    return jax.shard_map(
        local, mesh=mesh, in_specs=placed, out_specs=P("dp", "sp", None), check_vma=False)
```
